32 devices in a mesh: grp: 2 (over y), sp: 4 (over z), tp: 4 (over x, core).
Axes of the slice: x: 2, y: 2, z: 4, core: 2. Of those that a mesh axis runs over, the one named last changes fastest.
Arguments:
- stream: bfloat16 [2048, 4096], P(('grp', 'sp'), 'tp'), parts along dimension 0, may hold values from -6 to 6
- gain_pre: float32 [3, 4096], replicated, may hold values from 0.1 to 1.9
- w_in: bfloat16 [3, 4096, 1024], P(None, 'sp', 'tp'), may hold values from -0.09375 to 0.09375
- w_pool: bfloat16 [3, 4, 256, 256], P(None, 'tp'), may hold values from -0.375 to 0.375
- pool_scale: float32 [3, 1024], P(None, 'tp'), may hold values from 0.1 to 1.9
- w_out: bfloat16 [3, 1024, 4096], P(None, 'tp', 'sp'), may hold values from -0.5 to 0.5
- gain_post: float32 [3, 4096], replicated, may hold values from 0.1 to 1.9
Outputs:
- result: bfloat16 [2048, 4096], P(('grp', 'sp'), 'tp'), parts along dimension 0
The draws below stay inside these ranges and needn't reach their ends.
There are 2 independent parts, one for each index of `grp`. The reference program is written for one: setup_inputs(seed, part) draws one part's arguments, and reference() takes and returns one part's arrays. A program takes and returns all parts, laid end to end along the dimension named above; an argument that names none is the same for every part. Nothing has to cross between parts.
All inputs are finite; a program needn't handle non-finite values.
Results may differ from the reference program's by a relative error of at most 0.02.
Values may be sent and summed in bfloat16 or wider, within the bound.
A program may use at most 64 MiB of HBM per device.

```python
import jax
import jax.numpy as jnp
from jax import lax

D = 4096
GROUP = 256
POOL = 1024
LAYERS = 3
TOKENS = 1024


def draw_w_out(key, part):
    key_entries = jax.random.fold_in(key, 11)
    key_rough = jax.random.fold_in(key, 12)
    column_place = jnp.arange(D).astype(jnp.float32) / float(D - 1)
    rough = jax.random.uniform(key_rough, (D,), jnp.float32, 0.7, 1.4)
    entries = jax.random.normal(key_entries, (LAYERS, POOL, D), jnp.float32)
    column_scale = 0.4 * jnp.exp(jnp.log(6.0) * column_place) * rough
    values = entries * column_scale[None, None, :] * float(POOL) ** (-0.5)
    values = jnp.clip(values, -0.5, 0.5)
    return values.astype(jnp.bfloat16)


def block_levels(key, shape, pieces, low, high):
    level = 1.0
    for dim, parts in pieces:
        steps = jax.random.uniform(jax.random.fold_in(jax.random.fold_in(key, 6), dim), (parts,), jnp.float32, low / len(pieces), high / len(pieces))
        level = level * jnp.repeat(jnp.exp(steps), shape[dim] // parts).reshape((-1,) + (1,) * (len(shape) - 1 - dim))
    return level


def gaussian(rng, extent, deviation, most, shards=(), dtype=jnp.bfloat16):
    factor_of = block_levels(rng, extent, shards, -0.22, 0.18) if shards else 1.0
    values = jax.random.normal(rng, extent, jnp.float32) * deviation * factor_of
    return jnp.minimum(jnp.maximum(values, -most), most).astype(dtype)


def setup_inputs(seed: int = 0, part: int = 0) -> dict:
    arg_keys = jax.random.split(jax.random.key(seed), 8)
    part_keys = jax.random.split(jax.random.fold_in(arg_keys[7], part), 8)
    return {
        "stream": gaussian(part_keys[0], (TOKENS, D), 1.0, 6.0, ((0, 4), (1, 4))),
        "gain_pre": jnp.clip(1.0 + 0.18 * jax.random.normal(arg_keys[1], (LAYERS, D), jnp.float32), 0.1, 1.9),
        "w_in": gaussian(arg_keys[2], (LAYERS, D, POOL), D ** -0.5, 0.09375, ((1, 4), (2, 4))),
        "w_pool": gaussian(arg_keys[3], (LAYERS, 4, GROUP, GROUP), GROUP ** -0.5, 0.375, ((1, 4),)),
        "pool_scale": jnp.clip(1.0 + 0.18 * jax.random.normal(arg_keys[4], (LAYERS, POOL), jnp.float32), 0.1, 1.9),
        "w_out": draw_w_out(jax.random.fold_in(arg_keys[7], 71), part),
        "gain_post": jnp.clip(1.0 + 0.18 * jax.random.normal(arg_keys[6], (LAYERS, D), jnp.float32), 0.1, 1.9),
    }


WINDOWS = (2, 4, 8, 16)
EPS = 1e-06

def rms_scale(values, gain):
    inverse = lax.rsqrt(lax.optimization_barrier(jnp.mean(values * values, axis=-1, keepdims=True)) + EPS)
    return values * inverse * gain[None, :]

def reference(stream, gain_pre, w_in, w_pool, pool_scale, w_out, gain_post):
    reach = max(WINDOWS) - 1
    positions = jnp.arange(TOKENS).astype(jnp.float32)
    current = stream
    for layer in range(LAYERS):
        normed = rms_scale(current.astype(jnp.float32), gain_pre[layer]).astype(jnp.bfloat16)
        inner = jnp.dot(normed, w_in[layer], preferred_element_type=jnp.float32).astype(jnp.bfloat16)
        inner_f = inner.astype(jnp.float32)
        padded = jnp.concatenate([jnp.zeros((reach, 4 * GROUP), jnp.float32), inner_f], axis=0)
        branch = jnp.zeros((TOKENS, D), jnp.float32)
        for group_id in range(4):
            window = WINDOWS[group_id]
            lo = group_id * GROUP
            summed = jnp.zeros((TOKENS, GROUP), jnp.float32)
            for offset in range(window):
                summed = summed + padded[reach - offset:reach - offset + TOKENS, lo:lo + GROUP]
            count = jnp.minimum(positions + 1.0, float(window))
            pooled = summed / count[:, None]
            spread = (pooled - inner_f[:, lo:lo + GROUP]).astype(jnp.bfloat16)
            mixed = jnp.dot(spread, w_pool[layer, group_id], preferred_element_type=jnp.float32)
            mixed = (mixed * pool_scale[layer, lo:lo + GROUP][None, :]).astype(jnp.bfloat16)
            partial_value = jnp.dot(mixed, w_out[layer, lo:lo + GROUP], preferred_element_type=jnp.float32)
            partial_value = lax.optimization_barrier(partial_value.astype(jnp.bfloat16))
            branch = branch + partial_value.astype(jnp.float32)
        current = (current.astype(jnp.float32) + rms_scale(branch, gain_post[layer])).astype(jnp.bfloat16)
    return current
```

```python
import functools

import jax
import jax.numpy as jnp
from jax import lax
from jax.experimental import pallas as pl
from jax.experimental.pallas import tpu as pltpu
from jax.sharding import PartitionSpec as P

EPS = 1e-06
HALO = 16
CHUNKS = 4
PIECES = 2
PARTS = 4
PERIOD, STRIDE = 18, 2
AT_S, AT_B, AT_C, AT_F, AT_G, AT_D = 2.6, 6, 8, 10.3, 10.8, 13.5
LEAD, SPACE, RELAY, SECOND = 17.9, 1.5, 8, 4
MESH = pl.DeviceIdType.MESH
F32 = jnp.float32
BF16 = jnp.bfloat16


def kernel(
    G, S, T, layers, width,
    stream, gain_pre, w_in, w_pool, pool_scale, w_out, gain_post,
    out,
    win, wout, ag, part, pair, summed, xgot, normed, acc, ss, scale, branch, ext, halo, sq,
    load_sem, zs_sem, zr_sem, ys_sem, yr_sem,
    agp_sem, agx_sem, agr_sem, ps_sem, pr_sem, xs_sem, xr_sem, qs_sem, qr_sem, hs_sem, hr_sem,
):
    g, s, t = lax.axis_index("grp"), lax.axis_index("sp"), lax.axis_index("tp")
    pairs = T // 2
    p, c = lax.div(t, 2), lax.rem(t, 2)
    mate = p * 2 + 1 - c
    R, F = stream.shape
    group = w_pool.shape[2]
    rows_in, cols_out = w_in.shape[1], w_out.shape[2]
    per = S // T
    use_y = G == 2

    def remote(src, dst, send, recv, where):
        return pltpu.make_async_remote_copy(
            src_ref=src, dst_ref=dst, send_sem=send, recv_sem=recv,
            device_id=where, device_id_type=MESH,
        )

    def span(m, src, h):
        size = rows_in if m % 2 == 0 else group
        share = size // 2 if use_y else size
        length = share // PIECES
        start = (g * share if use_y else 0) + h * length
        if m % 2 == 0:
            return win.at[m // 2, pl.ds(pl.multiple_of(src * size + start, 16), length), :]
        return wout.at[m // 2, src, pl.ds(pl.multiple_of(start, 16), length), :]

    def z_copy(m, src, way, h):
        view = span(m, src, h)
        to = s + 1 if way == 0 else s - 1
        return remote(view, view, zs_sem.at[m, src, way, h], zr_sem.at[m, src, h], {"sp": to})

    def y_copy(m, src, h):
        view = span(m, src, h)
        return remote(view, view, ys_sem.at[m, src, h], yr_sem.at[m, src, h], {"grp": 1 - g})

    def load(m):
        if m % 2 == 0:
            return pltpu.make_async_copy(
                w_in.at[m // 2],
                win.at[m // 2, pl.ds(pl.multiple_of(s * rows_in, 16), rows_in), :],
                load_sem.at[m],
            )
        return pltpu.make_async_copy(w_out.at[m // 2], wout.at[m // 2, s], load_sem.at[m])

    M = 2 * layers

    def own(m):
        if m < M:
            load(m).wait()
            for h in range(PIECES):
                pl.when(s < S - 1)(lambda: z_copy(m, s, 0, h).start())
                pl.when(s > 0)(lambda: z_copy(m, s, 1, h).start())

    def relay(m, k, h):
        def from_left():
            src = s - 1 - k
            z_copy(m, src, 0, h).wait_recv()
            pl.when(s < S - 1)(lambda: z_copy(m, src, 0, h).start())
            if use_y:
                y_copy(m, src, h).start()

        def from_right():
            src = s + 1 + k
            z_copy(m, src, 1, h).wait_recv()
            pl.when(s > 0)(lambda: z_copy(m, src, 1, h).start())
            if use_y:
                y_copy(m, src, h).start()

        pl.when(s - 1 - k >= 0)(from_left)
        pl.when(s + 1 + k <= S - 1)(from_right)

    units = [(m, k, h) for m in range(M) for k in range(S - 1) for h in range(PIECES)]
    done = [0]

    def tick(n=1):
        for mm, k, h in units[done[0] : done[0] + n]:
            relay(mm, k, h)
            if k == min(1, S - 2) and h == PIECES - 1:
                own(mm + 1)
            done[0] += 1

    def pump(m):
        tick(max(0, (m + 1) * (S - 1) * PIECES - done[0]))

    def finish(m):
        if use_y:
            for src in range(S):
                for h in range(PIECES):
                    pl.when(s != src)(lambda: y_copy(m, src, h).wait_recv())

    def cut(l):
        return R // 2 - HALO * (layers - 1) + HALO * l

    def span_in(l, a):
        return (cut(l), R) if a == 0 else (0, cut(l))

    def span_out(l, a):
        return span_in(l + 1, a)

    def bits(bounds):
        lo, hi = bounds
        mid = lo + ((hi - lo) // 2 + 15) // 16 * 16
        return [(lo, mid), (mid, hi)]

    def sweep(bounds, body):
        lo, hi = bounds
        step = 32 if (hi - lo) % 32 == 0 else 16

        def one(i, carry):
            body(pl.ds(pl.multiple_of(lo + i * step, 16), step))
            return carry

        lax.fori_loop(0, (hi - lo) // step, one, 0)

    def lanes(x):
        return sum(x[:, i : i + 128] for i in range(0, F, 128))

    def ag_copy(l, block, a, i, sem, to):
        lo, hi = bits(span_in(l, a))[i]
        view = ag.at[l, block, pl.ds(lo, hi - lo), :]
        n = a * 2 + i
        return remote(view, view, sem, agr_sem.at[l, block, n], {"tp": to})

    def ag_start(l, a):
        for i in range(2):
            n = a * 2 + i
            for d in range(1, pairs):
                q = lax.rem(p + d, pairs)
                ag_copy(l, t, a, i, agx_sem.at[l, q, n], q * 2 + c).start()
        for i in range(2):
            ag_copy(l, t, a, i, agp_sem.at[l, p, a * 2 + i], mate).start()

    def ag_wait(l, block, a):
        for i in range(2):
            ag_copy(l, block, a, i, agp_sem.at[l, p, a * 2 + i], mate).wait_recv()

    def ag_relay(l, a):
        for d in range(1, pairs):
            q = lax.rem(p + d, pairs)
            for i in range(2):
                copy = ag_copy(l, q * 2 + c, a, i, agp_sem.at[l, q, a * 2 + i], mate)
                copy.wait_recv()
                copy.start()

    def absorb(l, block, a, first):
        lo, hi = span_in(l, a)
        gain = gain_pre[pl.ds(l, 1), pl.ds(pl.multiple_of(block * F, 128), F)]

        def body(rows):
            x = ag[l, block, rows, :].astype(F32)
            square = lanes(x * x)
            ss[rows, :] = square if first else ss[rows, :] + square
            normed[rows, :] = (x * gain).astype(BF16)

        sweep((lo, hi), body)
        product = jnp.dot(
            normed[lo:hi, :], win[l, pl.ds(pl.multiple_of(block * F, 128), F), :],
            preferred_element_type=F32,
        )
        acc[lo:hi, :] = product if first else acc[lo:hi, :] + product

    def inner(l, a):
        lo, hi = span_in(l, a)
        absorb(l, t, a, True)
        ag_wait(l, mate, a)
        absorb(l, mate, a, False)
        for d in range(1, pairs):
            q = lax.rem(p + d, pairs)
            absorb(l, q * 2 + c, a, False)
            ag_wait(l, q * 2 + 1 - c, a)
            absorb(l, q * 2 + 1 - c, a, False)
        inverse = lax.rsqrt(jnp.sum(ss[lo:hi, :], axis=1, keepdims=True) / width + EPS)
        ext[l, HALO + lo : HALO + hi, :] = (acc[lo:hi, :] * inverse).astype(BF16)

    def halo_copy(l):
        return remote(
            ext.at[l, pl.ds(R, HALO), :], halo.at[l], hs_sem.at[l], hr_sem.at[l], {"sp": s + 1}
        )

    def halo_in(l):
        pl.when(s > 0)(lambda: halo_copy(l).wait_recv())

        @pl.when(s == 0)
        def _():
            ext[l, pl.ds(0, HALO), :] = jnp.zeros((HALO, group), BF16)

        @pl.when(s > 0)
        def _():
            ext[l, pl.ds(0, HALO), :] = halo[l]

    def pool(l, a):
        lo, hi = span_out(l, a)
        values = ext[l, lo : hi + HALO, :].astype(F32)
        two = values + pltpu.roll(values, 1, 0)
        four = two + pltpu.roll(two, 2, 0)
        eight = four + pltpu.roll(four, 4, 0)
        sixteen = eight + pltpu.roll(eight, 8, 0)
        total = jnp.where(t == 0, two, jnp.where(t == 1, four, jnp.where(t == 2, eight, sixteen)))
        window = jnp.where(t == 0, 2, jnp.where(t == 1, 4, jnp.where(t == 2, 8, 16)))
        place = s * R + lo + lax.broadcasted_iota(jnp.int32, (hi - lo, group), 0)
        count = jnp.minimum(place + 1, window).astype(F32)
        spread = (total[HALO:, :] / count - values[HALO:, :]).astype(BF16)
        mixed = jnp.dot(spread, w_pool[l, 0], preferred_element_type=F32)
        return (mixed * pool_scale[l : l + 1, :]).astype(BF16)

    def project(l, a, dest, mixed):
        lo, hi = span_out(l, a)
        for k in range(per):
            value = jnp.dot(mixed, wout[l, dest * per + k], preferred_element_type=F32)
            part[l, dest, lo:hi, k * cols_out : (k + 1) * cols_out] = value.astype(BF16)

    def pair_copy(l, q, a, i):
        lo, hi = bits(span_out(l, a))[i]
        rows, n = pl.ds(lo, hi - lo), a * 2 + i
        return remote(
            part.at[l, q * 2 + 1 - c, rows, :], pair.at[l, q, rows, :],
            ps_sem.at[l, q, n], pr_sem.at[l, q, n], {"tp": mate},
        )

    def cross_copy(l, q, slot, a, i):
        lo, hi = bits(span_out(l, a))[i]
        rows, n = pl.ds(lo, hi - lo), a * 2 + i
        return remote(
            summed.at[l, q, rows, :], xgot.at[l, slot, rows, :],
            xs_sem.at[l, q, n], xr_sem.at[l, slot, n], {"tp": q * 2 + c},
        )

    def scatter_first(l, a, mixed):
        for d in range(1, pairs):
            q = lax.rem(p + d, pairs)
            project(l, a, q * 2 + 1 - c, mixed)
            for i in range(2):
                pair_copy(l, q, a, i).start()
        for d in range(1, pairs):
            project(l, a, lax.rem(p + d, pairs) * 2 + c, mixed)

    def scatter_cross(l, a):
        for d in range(1, pairs):
            q = lax.rem(p + d, pairs)
            for i in range(2):
                pair_copy(l, q, a, i).wait_recv()

                def body(rows):
                    summed[l, q, rows, :] = (
                        part[l, q * 2 + c, rows, :].astype(F32) + pair[l, q, rows, :].astype(F32)
                    ).astype(BF16)

                sweep(bits(span_out(l, a))[i], body)
                cross_copy(l, q, p, a, i).start()

    def scatter_own(l, a, mixed):
        project(l, a, mate, mixed)
        for i in range(2):
            pair_copy(l, p, a, i).start()
        project(l, a, t, mixed)

    def sq_copy(l, slot, a, to):
        view = sq.at[l, a, slot]
        return remote(view, view, qs_sem.at[l, a, to], qr_sem.at[l, a, slot], {"tp": to})

    def settle(l, a):
        for i in range(2):
            pair_copy(l, p, a, i).wait_recv()
            for d in range(1, pairs):
                q = lax.rem(p + d, pairs)
                cross_copy(l, q, q, a, i).wait_recv()

            def add(rows):
                value = part[l, t, rows, :].astype(F32) + pair[l, p, rows, :].astype(F32)
                for d in range(1, pairs):
                    value = value + xgot[l, lax.rem(p + d, pairs), rows, :].astype(F32)
                branch[rows, :] = value
                ss[rows, :] = lanes(value * value)

            sweep(bits(span_out(l, a))[i], add)
        row = jnp.sum(jnp.transpose(ss[...]), axis=0, keepdims=True)
        sq[l, a, t] = jnp.broadcast_to(row, (8, R))
        for d in range(1, T):
            sq_copy(l, t, a, lax.rem(t + d, T)).start()
        tick()
        for d in range(1, T):
            other = lax.rem(t + d, T)
            sq_copy(l, other, a, other).wait_recv()
        squares = sq[l, a, 0]
        for k in range(1, T):
            squares = squares + sq[l, a, k]
        inverse = lax.rsqrt(squares / width + EPS)
        scale[...] = jnp.transpose(jnp.concatenate([inverse] * 16, axis=0))
        gain = gain_post[pl.ds(l, 1), pl.ds(pl.multiple_of(t * F, 128), F)]

        def update(rows):
            value = ag[l, t, rows, :].astype(F32) + branch[rows, :] * scale[rows, 0:1] * gain
            if l + 1 < layers:
                ag[l + 1, t, rows, :] = value.astype(BF16)
            else:
                out[rows, :] = value.astype(BF16)

        sweep(span_out(l, a), update)
        if l + 1 < layers:
            ag_start(l + 1, a)

    for m in range(M):
        load(m).start()
    barrier = pltpu.get_barrier_semaphore()

    def greet(where):
        pl.semaphore_signal(barrier, inc=1, device_id=where, device_id_type=MESH)

    pl.when(s < S - 1)(lambda: greet({"sp": s + 1}))
    pl.when(s > 0)(lambda: greet({"sp": s - 1}))
    if use_y:
        greet({"grp": 1 - g})
    for d in range(1, T):
        greet({"tp": lax.rem(t + d, T)})
    ag[0, t] = stream[...]
    ends = jnp.where(s > 0, 1, 0) + jnp.where(s < S - 1, 1, 0)
    pl.semaphore_wait(barrier, ends + (1 if use_y else 0) + T - 1)

    own(0)
    ag_start(0, 0)
    ag_start(0, 1)
    each = (S - 1) * PIECES
    for l in range(layers):
        if l == 0:
            tick(each // 3)
            ag_relay(0, 0)
            tick(each // 3)
            ag_relay(0, 1)
        else:
            ag_relay(l, 0)
        pump(2 * l)
        finish(2 * l)
        inner(l, 0)
        pl.when(s < S - 1)(lambda: halo_copy(l).start())
        mixed = pool(l, 0)
        if l == 0:
            tick()
            inner(l, 1)
            tick()
            halo_in(l)
            later = pool(l, 1)
        pump(2 * l + 1)
        finish(2 * l + 1)
        scatter_first(l, 0, mixed)
        tick()
        if l > 0:
            ag_relay(l, 1)
        scatter_cross(l, 0)
        tick()
        scatter_own(l, 0, mixed)
        tick()
        if l > 0:
            inner(l, 1)
            tick()
            halo_in(l)
            later = pool(l, 1)
        scatter_first(l, 1, later)
        tick()
        scatter_cross(l, 1)
        tick()
        scatter_own(l, 1, later)
        tick()
        settle(l, 0)
        tick()
        settle(l, 1)
        tick()

    for l in range(layers):
        pl.when(s < S - 1)(lambda: halo_copy(l).wait_send())
        for a in range(2):
            for d in range(1, T):
                sq_copy(l, t, a, lax.rem(t + d, T)).wait_send()
            for i in range(2):
                n = a * 2 + i
                for q in range(pairs):
                    ag_copy(l, t, a, i, agp_sem.at[l, q, n], mate).wait_send()
                    pair_copy(l, q, a, i).wait_send()
                for d in range(1, pairs):
                    q = lax.rem(p + d, pairs)
                    ag_copy(l, t, a, i, agx_sem.at[l, q, n], mate).wait_send()
                    cross_copy(l, q, p, a, i).wait_send()
    for m in range(M):
        for src in range(S):
            for h in range(PIECES):
                pl.when(jnp.logical_and(src <= s, s < S - 1))(lambda: z_copy(m, src, 0, h).wait_send())
                pl.when(jnp.logical_and(src >= s, s > 0))(lambda: z_copy(m, src, 1, h).wait_send())
                if use_y:
                    pl.when(s != src)(lambda: y_copy(m, src, h).wait_send())


def per_device(G, S, T, stream, gain_pre, w_in, w_pool, pool_scale, w_out, gain_post):
    layers, width = gain_pre.shape
    R, F = stream.shape
    group = w_pool.shape[2]
    pairs = T // 2
    M = 2 * layers
    dma = pltpu.SemaphoreType.DMA
    vmem = pl.BlockSpec(memory_space=pltpu.VMEM)
    anywhere = pl.BlockSpec(memory_space=pl.ANY)
    return pl.pallas_call(
        functools.partial(kernel, G, S, T, layers, width),
        out_shape=jax.ShapeDtypeStruct((R, F), BF16),
        in_specs=[vmem, vmem, anywhere, vmem, vmem, anywhere, vmem],
        out_specs=vmem,
        scratch_shapes=[
            pltpu.VMEM((layers, width, group), BF16),
            pltpu.VMEM((layers, S, group, w_out.shape[2]), BF16),
            pltpu.VMEM((layers, T, R, F), BF16),
            pltpu.VMEM((layers, T, R, F), BF16),
            pltpu.VMEM((layers, pairs, R, F), BF16),
            pltpu.VMEM((layers, pairs, R, F), BF16),
            pltpu.VMEM((layers, pairs, R, F), BF16),
            pltpu.VMEM((R, F), BF16),
            pltpu.VMEM((R, group), F32),
            pltpu.VMEM((R, 128), F32),
            pltpu.VMEM((R, 128), F32),
            pltpu.VMEM((R, F), F32),
            pltpu.VMEM((layers, HALO + R, group), BF16),
            pltpu.VMEM((layers, HALO, group), BF16),
            pltpu.VMEM((layers, 2, T, 8, R), F32),
            dma((M,)),
            dma((M, S, 2, PIECES)),
            dma((M, S, PIECES)),
            dma((M, S, PIECES)),
            dma((M, S, PIECES)),
            dma((layers, pairs, CHUNKS)),
            dma((layers, pairs, CHUNKS)),
            dma((layers, T, CHUNKS)),
            dma((layers, pairs, CHUNKS)),
            dma((layers, pairs, CHUNKS)),
            dma((layers, pairs, CHUNKS)),
            dma((layers, pairs, CHUNKS)),
            dma((layers, 2, T)),
            dma((layers, 2, T)),
            dma((layers,)),
            dma((layers,)),
        ],
        compiler_params=pltpu.CompilerParams(
            collective_id=0, has_side_effects=True, vmem_limit_bytes=60 * 1024 * 1024
        ),
    )(stream, gain_pre, w_in, w_pool, pool_scale, w_out, gain_post)


def plane_kernel(
    G, S, T, layers, width, order,
    stream_hbm, gain_pre_hbm, w_in, w_pool, scale_hbm, w_out, gain_post_hbm,
    out,
    stream, gain_pre, gain_post, win, wout, wp, scales, rows_in, x,
    part, got, far, psq, ext, mix, branch, bsq,
    load_sem, small_sem, self_sem, y_send, y_recv, x_send, x_recv, f_send, f_recv,
    wo_send, wo_recv, wx_send, wx_recv, wy_send, wy_recv, wf_send, wf_recv,
    p_send, p_recv, c_send, c_recv,
    r_send, r_recv, o_send, o_recv, rq_send, rq_recv, h_send, h_recv, m_send, m_recv, mq_send, mq_recv,
):
    g, s, t = lax.axis_index("grp"), lax.axis_index("sp"), lax.axis_index("tp")
    pairs = T // 2
    p, c = lax.div(t, 2), lax.rem(t, 2)
    mate = p * 2 + 1 - c
    R, F = stream.shape
    C = R // T
    group = w_pool.shape[2]
    sides = 2 if G == 2 else 1
    side = g if sides == 2 else 0
    M = 2 * layers
    line_width = psq.shape[-1]
    H = S // 2
    low = lax.div(s, H) * H
    here = s - low
    hub, far_hub = jnp.where(low == 0, H - 1, H), jnp.where(low == 0, H, H - 1)
    is_hub = s == hub
    near = [low + lax.rem(here + d, H) for d in range(1, H)]
    away = [H - low + d for d in range(H)]
    planes = near + away

    def slot(k):
        return lax.rem(k - low + S, S)

    def remote(src, dst, send, recv, where):
        return pltpu.make_async_remote_copy(
            src_ref=src, dst_ref=dst, send_sem=send, recv_sem=recv,
            device_id=where, device_id_type=MESH,
        )

    def sent(view, sem):
        remote(view, view, sem, sem, {"tp": mate}).wait_send()

    def landed(view, sem):
        remote(view, view, sem, sem, {"tp": mate}).wait_recv()

    barrier = pltpu.get_barrier_semaphore()

    def greet(where):
        pl.semaphore_signal(barrier, inc=1, device_id=where, device_id_type=MESH)

    for ds in range(S):
        for dt in range(T):
            if ds or dt:
                greet({"sp": lax.rem(s + ds, S), "tp": lax.rem(t + dt, T)})
    if sides == 2:
        greet({"grp": 1 - g})

    smalls = [
        pltpu.make_async_copy(stream_hbm, stream, small_sem.at[0]),
        pltpu.make_async_copy(gain_pre_hbm, gain_pre, small_sem.at[1]),
        pltpu.make_async_copy(gain_post_hbm, gain_post, small_sem.at[2]),
    ]
    scale_load = pltpu.make_async_copy(scale_hbm, scales, small_sem.at[3])

    def block(m, k):
        if m % 2 == 0:
            return win.at[m // 2, slot(k)]
        return wout.at[m // 2, pl.ds(pl.multiple_of(slot(k) * group, 16), group), :]

    def piece(m, k, half, h):
        rows = (F if m % 2 == 0 else group) // sides
        length = rows // PARTS
        start = half * rows + h * length
        if m % 2 == 0:
            return win.at[m // 2, slot(k), pl.ds(pl.multiple_of(start, 16), length), :]
        return wout.at[m // 2, pl.ds(pl.multiple_of(slot(k) * group + start, 16), length), :]

    def load(m):
        return pltpu.make_async_copy((w_out if m % 2 else w_in).at[m // 2], block(m, t), load_sem.at[m])

    def own_copy(m, k):
        return remote(block(m, k), block(m, k), wo_send.at[m], wo_recv.at[m], {"tp": mate})

    def cross_copy(m, k, d, q, h):
        view = piece(m, k, side, h)
        return remote(view, view, wx_send.at[m, d], wx_recv.at[m, d, h], {"tp": q * 2 + c})

    def grp_copy(m, d, q, half, h):
        view = piece(m, q * 2 + c, half, h)
        return remote(view, view, wy_send.at[m, d], wy_recv.at[m, d, h], {"grp": 1 - g})

    def mate_copy(m, d, q, half, h):
        view = piece(m, q * 2 + c, half, h)
        return remote(view, view, wf_send.at[m, d], wf_recv.at[m, d], {"tp": mate})

    others = [(d, lax.rem(p + 1 + d, pairs)) for d in range(pairs - 1)]

    def weight_own(m):
        load(m).wait()
        own_copy(m, t).start()

    def weight_cross(m, h):
        for d, q in others:
            back = pairs - 2 - d
            view = piece(m, t, side, h)
            remote(view, view, wx_send.at[m, d], wx_recv.at[m, back, h], {"tp": q * 2 + c}).start()

    def weight_relay(m, h):
        for d, q in others:
            cross_copy(m, q * 2 + c, d, q, h).wait_recv()
            if sides == 2:
                grp_copy(m, d, q, side, h).start()
            mate_copy(m, d, q, side, h).start()

    def weight_second(m, h):
        if sides == 2:
            for d, q in others:
                grp_copy(m, d, q, 1 - side, h).wait_recv()
                mate_copy(m, d, q, 1 - side, h).start()

    def weight_last(m):
        for d, q in others:
            landed(block(m, q * 2 + 1 - c), wf_recv.at[m, d])

    def share(m, k):
        rows = (F if m % 2 == 0 else group) // sides
        if m % 2 == 0:
            return win.at[m // 2, slot(k), pl.ds(0, rows), :]
        return wout.at[m // 2, pl.ds(pl.multiple_of(slot(k) * group, 16), rows), :]

    def pool_copy(l, d):
        return remote(wp.at[l], wp.at[l], p_send.at[d - 1], p_recv.at[l], {"tp": lax.rem(t + d, T)})

    def scale_copy(d):
        return remote(scales, scales, c_send.at[d - 1], c_recv, {"tp": lax.rem(t + d, T)})

    def pool_send(l):
        @pl.when(t == s)
        def _():
            for d in range(1, T):
                pool_copy(l, d).start()

    def lanes(v):
        return sum(v[:, i : i + 128] for i in range(0, F, 128))

    def line(square):
        if C < line_width:
            square = jnp.concatenate([square, jnp.zeros((line_width - C, 128), F32)], axis=0)
        row = jnp.sum(jnp.transpose(square), axis=0, keepdims=True)
        return jnp.broadcast_to(row, (8, line_width))

    def column(values):
        return jnp.transpose(jnp.concatenate([values] * 16, axis=0))[:C]

    def wide(values, n):
        return jnp.concatenate([values] * (n // 128), axis=1)

    def squares_start(ref, l, q, send, recv):
        for d in range(1, S):
            remote(ref.at[l, q, 0], ref.at[l, q, d], send, recv.at[l, q], {"sp": lax.rem(s + d, S)}).start()

    def squares_wait(ref, l, q, recv):
        landed(ref.at[l, q, pl.ds(1, S - 1)], recv.at[l, q])

    def total(ref, l, q):
        return sum(ref[l, q, k] for k in range(S))

    def halo_copy(l, q):
        ahead = q + lax.div(t + 1, T)
        return remote(
            ext.at[l, q, pl.ds(C, HALO), :], ext.at[l, ahead, pl.ds(0, HALO), :],
            h_send.at[1 if q + 1 == S else 0], h_recv.at[l, ahead], {"tp": lax.rem(t + 1, T)},
        )

    def run_copy(to, origin):
        rows = pl.ds(pl.multiple_of(to * C, 16), C)
        return remote(stream.at[rows, :], rows_in.at[origin], y_send, y_recv.at[origin], {"tp": to})

    def run_of(f, local):
        return stream.at[pl.ds(pl.multiple_of(t * C, 16), C), :] if local else rows_in.at[f]

    def stream_self(local):
        return pltpu.make_async_copy(run_of(s, local), x.at[s], self_sem.at[0])

    def stream_on(f, local=False):
        pl.when(f == s)(lambda: stream_self(local).start())
        pl.when(f != s)(
            lambda: remote(run_of(f, local), x.at[s], x_send, x_recv.at[s], {"sp": f}).start()
        )

    def final_copy(q):
        rows = pl.ds(pl.multiple_of(t * C, 16), C)
        return remote(x.at[q], out.at[rows, :], f_send, f_recv, {"sp": q, "tp": s})

    def final_self(q):
        rows = pl.ds(pl.multiple_of(t * C, 16), C)
        return pltpu.make_async_copy(x.at[q], out.at[rows, :], self_sem.at[1])

    def features(ref, l):
        return ref[pl.ds(l, 1), pl.ds(pl.multiple_of(s * F, 128), F)]

    def stage_a(l, q):
        with jax.named_scope(f"a{l}{q}"):
            advance(l, q)

    def advance(l, q):
        if l == 0:
            pl.when(s == q)(lambda: stream_self(False).wait())
            pl.when(s != q)(lambda: landed(x.at[q], x_recv.at[q]))
            value = x[q].astype(F32)
        else:
            squares_wait(bsq, l - 1, q, mq_recv)
            inverse = column(lax.rsqrt(total(bsq, l - 1, q) / width + EPS))
            new = x[q].astype(F32) + branch[q] * wide(inverse, F) * features(gain_post, l - 1)
            new = new.astype(BF16)
            x[q] = new
            if l == layers:
                mine = jnp.logical_and(s == q, t == s)
                pl.when(mine)(lambda: final_self(q).start())
                pl.when(jnp.logical_not(mine))(lambda: final_copy(q).start())
                return
            value = new.astype(F32)
        psq[l, q, 0] = line(lanes(value * value))
        squares_start(psq, l, q, rq_send, rq_recv)
        scaled = (value * features(gain_pre, l)).astype(BF16)

        def project(k):
            part[l, q, k] = jnp.dot(scaled, win[l, k], preferred_element_type=F32).astype(BF16)

        if q == 0 and l == 0:
            project(slot(t))
            landed(block(0, mate), wo_recv.at[0])
            project(slot(mate))
            for h in range(PARTS):
                weight_relay(0, h)
            for h in range(PARTS):
                weight_second(0, h)
            for _, d in others:
                project(slot(d * 2 + c))
            weight_last(0)
            for _, d in others:
                project(slot(d * 2 + 1 - c))
            outward(l, q)
            inward(l, q)
        else:
            if q == 0:
                ready(2 * l)
            for k in range(H, S):
                project(k)
            outward(l, q)
            for k in range(H):
                project(k)
            inward(l, q)

    def outward(l, q):
        @pl.when(jnp.logical_not(is_hub))
        def _():
            index = jnp.where(here > hub - low, here - 1, here)
            remote(
                part.at[l, q, pl.ds(H, H)], far.at[l, q, index], o_send, o_recv.at[l, q], {"sp": hub}
            ).start()

    def inward(l, q):
        for d, k in enumerate(near):
            remote(
                part.at[l, q, slot(k)], got.at[l, q, H - 2 - d], r_send, r_recv.at[l, q], {"sp": k}
            ).start()

    def stage_s(l, q):
        with jax.named_scope(f"s{l}{q}"):

            @pl.when(is_hub)
            def _():
                landed(far.at[l, q], o_recv.at[l, q])
                for k in range(H):
                    value = part[l, q, H + k].astype(F32)
                    for d in range(H - 1):
                        value = value + far[l, q, d, k].astype(F32)
                    part[l, q, H + k] = value.astype(BF16)
                    remote(
                        part.at[l, q, H + k], got.at[l, q, H - 1], o_send, r_recv.at[l, q], {"sp": away[k]}
                    ).start()

    def ready(m):
        landed(block(m, mate), wo_recv.at[m])
        weight_last(m)

    def stage_b(l, q):
        with jax.named_scope(f"b{l}{q}"):
            squares_wait(psq, l, q, rq_recv)
            inverse = column(lax.rsqrt(total(psq, l, q) / width + EPS))
            landed(got.at[l, q], r_recv.at[l, q])
            value = part[l, q, here].astype(F32)
            for k in range(H):
                value = value + got[l, q, k].astype(F32)
            ext[l, q, HALO:, :] = (value * wide(inverse, group)).astype(BF16)
            if q + 1 < S:
                halo_copy(l, q).start()
            else:
                pl.when(t + 1 < T)(lambda: halo_copy(l, q).start())

    def halo_wait(l, q):
        landed(ext.at[l, q, pl.ds(0, HALO), :], h_recv.at[l, q])

    def stage_c(l, q):
        with jax.named_scope(f"c{l}{q}"):
            smooth(l, q)

    def smooth(l, q):
        if q == 0:
            pl.when(t > 0)(lambda: halo_wait(l, q))

            @pl.when(t == 0)
            def _():
                ext[l, q, pl.ds(0, HALO), :] = jnp.zeros((HALO, group), BF16)

            pl.when(t != s)(lambda: landed(wp.at[l], p_recv.at[l]))
            if l == 0:
                pl.when(t != s)(lambda: landed(scales, c_recv))
        else:
            halo_wait(l, q)
        values = ext[l, q].astype(F32)
        reach = values
        pooled = values
        for k in range(S):
            reach = reach + pltpu.roll(reach, 2**k, 0)
            pooled = jnp.where(s == k, reach, pooled)
        window = jnp.left_shift(2, s)
        place = q * R + t * C + lax.broadcasted_iota(jnp.int32, (C, group), 0)
        count = jnp.minimum(place + 1, window).astype(F32)
        spread = (pooled[HALO:, :] / count - values[HALO:, :]).astype(BF16)
        mixed = jnp.dot(spread, wp[l], preferred_element_type=F32)
        mix[l, q, here] = (mixed * scales[l : l + 1, :]).astype(BF16)

        def on(k, kind):
            lower = lax.div(k, H) * H
            remote(
                mix.at[l, q, here], mix.at[l, q, lax.rem(s - lower + S, S)],
                m_send.at[3 if kind else 0], m_recv.at[kind, l, q], {"sp": k},
            ).start()

        for k in near:
            on(k, 0)
        pl.when(is_hub)(lambda: on(far_hub, 1))

    def mates_view(l, q):
        return mix.at[l, q, pl.ds(0, H - 1)]

    def stage_f(l, q):
        with jax.named_scope(f"f{l}{q}"):

            @pl.when(is_hub)
            def _():
                landed(mates_view(l, q), m_recv.at[0, l, q])
                for j in range(1, H):
                    from_here = lax.rem(here + j, H)
                    for k in away:
                        remote(
                            mix.at[l, q, from_here], mix.at[l, q, H + from_here],
                            m_send.at[1], m_recv.at[2, l, q], {"sp": k},
                        ).start()

    def stage_g(l, q):
        with jax.named_scope(f"g{l}{q}"):

            @pl.when(is_hub)
            def _():
                spot = slot(far_hub)
                landed(mix.at[l, q, spot], m_recv.at[1, l, q])
                for k in near:
                    remote(
                        mix.at[l, q, spot], mix.at[l, q, spot],
                        m_send.at[2], m_recv.at[1, l, q], {"sp": k},
                    ).start()

    def stage_d(l, q):
        with jax.named_scope(f"d{l}{q}"):
            if q == 0:
                ready(2 * l + 1)

            @pl.when(jnp.logical_not(is_hub))
            def _():
                landed(mates_view(l, q), m_recv.at[0, l, q])
                landed(mix.at[l, q, 0], m_recv.at[1, l, q])

            landed(mates_view(l, q), m_recv.at[2, l, q])
            value = jnp.dot(
                jnp.concatenate([mix[l, q, k] for k in range(S)], axis=1), wout[l],
                preferred_element_type=F32,
            )
            branch[q] = value
            bsq[l, q, 0] = line(lanes(value * value))
            squares_start(bsq, l, q, mq_send, mq_recv)

    smalls[0].start()
    for m in range(M):
        load(m).start()
    smalls[1].start()
    smalls[2].start()
    pool_load = [pltpu.make_async_copy(w_pool.at[l, 0], wp.at[l], p_recv.at[l]) for l in range(layers)]

    @pl.when(t == s)
    def _():
        for l in range(layers):
            pool_load[l].start()
        scale_load.start()

    smalls[0].wait()
    pl.semaphore_wait(barrier, S * T - 1 + (1 if sides == 2 else 0))

    for _, q in others:
        run_copy(q * 2 + c, t).start()
        run_copy(q * 2 + 1 - c, t).start()
    run_copy(mate, t).start()
    stream_on(t, True)
    weight_own(0)
    for h in range(PARTS):
        weight_cross(0, h)
    weight_own(1)
    for h in range(PARTS):
        weight_cross(1, h)
    with jax.named_scope("enter"):
        landed(rows_in.at[mate], y_recv.at[mate])
        stream_on(mate)
        for _, q in others:
            for core in (c, 1 - c):
                landed(rows_in.at[q * 2 + core], y_recv.at[q * 2 + core])
                stream_on(q * 2 + core)

    @pl.when(t == s)
    def _():
        for l in range(layers):
            pool_load[l].wait()
        scale_load.wait()
        for d in range(1, T):
            scale_copy(d).start()

    pool_send(0)
    smalls[1].wait()
    smalls[2].wait()

    actions = (
        stage_a, stage_b, stage_c, stage_d, weight_own, pool_send, weight_cross, weight_relay, weight_second,
        stage_s, stage_f, stage_g,
    )
    for kind, *where in order:
        actions[kind](*where)

    rows = pl.ds(0, (T - 1) * C)

    @pl.when(s == t)
    def _():
        final_self(s).wait()
        landed(out.at[rows, :], f_recv)
        sent(out.at[rows, :], f_send)

    @pl.when(s != t)
    def _():
        landed(out, f_recv)
        sent(out, f_send)

    with jax.named_scope("drain"):
        sent(stream.at[rows, :], y_send)
        sent(x.at[pl.ds(0, S - 1)], x_send)

        @pl.when(t == s)
        def _():
            for d in range(1, T):
                sent(scales, c_send.at[d - 1])
                sent(wp, p_send.at[d - 1])

        for m in range(M):
            sent(block(m, t), wo_send.at[m])
            for d, q in others:
                sent(share(m, t), wx_send.at[m, d])
                sent(block(m, t), wf_send.at[m, d])
                if sides == 2:
                    sent(share(m, t), wy_send.at[m, d])
        sent(psq.at[:, :, pl.ds(0, S - 1)], rq_send)
        sent(bsq.at[:, :, pl.ds(0, S - 1)], mq_send)
        sent(part.at[:, :, pl.ds(0, H - 1)], r_send)
        sent(part.at[:, :, pl.ds(0, H)], o_send)
        sent(mix.at[:, :, pl.ds(0, H - 1)], m_send.at[0])

        @pl.when(is_hub)
        def _():
            sent(mix.at[:, :, 0], m_send.at[3])
            sent(mix.at[:, :, pl.ds(0, (H - 1) * H)], m_send.at[1])
            sent(mix.at[:, :, pl.ds(0, H - 1)], m_send.at[2])

        sent(ext.at[:, pl.ds(0, S - 1), pl.ds(0, HALO), :], h_send.at[0])
        pl.when(t + 1 < T)(lambda: sent(ext.at[:, 0, pl.ds(0, HALO), :], h_send.at[1]))


def stage_order(layers, runs):
    steps = []
    begins = {0: 0, 9: AT_S, 1: AT_B, 2: AT_C, 10: AT_F, 11: AT_G, 3: AT_D}
    for l in range(layers + 1):
        for kind, at in begins.items():
            if l < layers or kind == 0:
                for q in range(runs):
                    steps.append((l * PERIOD + at + q * STRIDE, (kind, l, q)))
    for m in range(1, 2 * layers):
        due = m // 2 * PERIOD + (AT_D if m % 2 else 0) - 0.1
        begin = due - LEAD
        if m == 1:
            begin = due - (PARTS - 1) * SPACE - RELAY - SECOND
        for h in range(PARTS):
            if m > 1:
                if h == 0:
                    steps.append((begin, (4, m)))
                    if m % 2 == 0:
                        steps.append((begin, (5, m // 2)))
                steps.append((begin + h * SPACE, (6, m, h)))
            steps.append((begin + h * SPACE + RELAY, (7, m, h)))
            steps.append((begin + h * SPACE + RELAY + SECOND, (8, m, h)))
    return [step for _, step in sorted(steps)]


def per_plane(G, S, T, stream, gain_pre, w_in, w_pool, pool_scale, w_out, gain_post):
    layers, width = gain_pre.shape
    R, F = stream.shape
    group = w_pool.shape[2]
    C = R // T
    H = S // 2
    pairs = T // 2
    M = 2 * layers
    wide = max(128, C)
    dma = pltpu.SemaphoreType.DMA
    anywhere = pl.BlockSpec(memory_space=pl.ANY)
    return pl.pallas_call(
        functools.partial(plane_kernel, G, S, T, layers, width, stage_order(layers, S)),
        out_shape=jax.ShapeDtypeStruct((R, F), BF16),
        in_specs=[anywhere] * 7,
        out_specs=pl.BlockSpec(memory_space=pltpu.VMEM),
        scratch_shapes=[
            pltpu.VMEM((R, F), BF16),
            pltpu.VMEM((layers, width), F32),
            pltpu.VMEM((layers, width), F32),
            pltpu.VMEM((layers, T, F, group), BF16),
            pltpu.VMEM((layers, T * group, F), BF16),
            pltpu.VMEM((layers, group, group), BF16),
            pltpu.VMEM((layers, group), F32),
            pltpu.VMEM((T, C, F), BF16),
            pltpu.VMEM((S, C, F), BF16),
            pltpu.VMEM((layers, S, S, C, group), BF16),
            pltpu.VMEM((layers, S, H, C, group), BF16),
            pltpu.VMEM((layers, S, H - 1, H, C, group), BF16),
            pltpu.VMEM((layers, S, S, 8, wide), F32),
            pltpu.VMEM((layers, S, HALO + C, group), BF16),
            pltpu.VMEM((layers, S, S, C, group), BF16),
            pltpu.VMEM((S, C, F), F32),
            pltpu.VMEM((layers, S, S, 8, wide), F32),
            dma((M,)),
            dma((4,)),
            dma((2,)),
            dma(()),
            dma((T,)),
            dma(()),
            dma((S,)),
            dma(()),
            dma(()),
            dma((M,)),
            dma((M,)),
            dma((M, pairs - 1)),
            dma((M, pairs - 1, PARTS)),
            dma((M, pairs - 1)),
            dma((M, pairs - 1, PARTS)),
            dma((M, pairs - 1)),
            dma((M, pairs - 1)),
            dma((T - 1,)),
            dma((layers,)),
            dma((T - 1,)),
            dma(()),
            dma(()),
            dma((layers, S)),
            dma(()),
            dma((layers, S)),
            dma(()),
            dma((layers, S)),
            dma((2,)),
            dma((layers, S)),
            dma((4,)),
            dma((3, layers, S)),
            dma(()),
            dma((layers, S)),
        ],
        compiler_params=pltpu.CompilerParams(
            collective_id=0, has_side_effects=True, vmem_limit_bytes=60 * 1024 * 1024
        ),
    )(stream, gain_pre, w_in, w_pool, pool_scale, w_out, gain_post)


def plan(G, S, T, *args):
    stream, w_pool = args[0], args[3]
    planes = S == T == T * w_pool.shape[1] and 2 < S and 2**S <= HALO and S % 2 == 0 and stream.shape[0] % (HALO * T) == 0
    return (per_plane if planes else per_device)(G, S, T, *args)


def solution(mesh):
    G, S, T = mesh.shape["grp"], mesh.shape["sp"], mesh.shape["tp"]
    return jax.shard_map(
        functools.partial(plan, G, S, T),
        mesh=mesh,
        in_specs=(
            P(("grp", "sp"), "tp"),
            P(),
            P(None, "sp", "tp"),
            P(None, "tp", None, None),
            P(None, "tp"),
            P(None, "tp", "sp"),
            P(),
        ),
        out_specs=P(("grp", "sp"), "tp"),
        check_vma=False,
    )
```

```python
import functools

import jax
import jax.numpy as jnp
from jax import lax
from jax.experimental import pallas as pl
from jax.experimental.pallas import tpu as pltpu
from jax.sharding import PartitionSpec as P

EPS = 1e-06
HALO = 16
CHUNKS = 4
PIECES = 2
PARTS = 4
RELAYED = True
OUT_SPEC = pl.BlockSpec(memory_space=pl.ANY)
PERIOD, STRIDES = 17, (2, 2.5, 2.5)
AT_S, AT_B, AT_F, AT_G, AT_D, AT_Z = 3, 6.2, 9.6, 9.7, 13, 0
EARLY = (1.5, 0.75)
SPACE, LEADS, RELAYS, SECONDS, FIRST = 1.5, (16.9, 16.9), (8, 8), (4, 4), (8, 4)
MESH = pl.DeviceIdType.MESH
F32 = jnp.float32
BF16 = jnp.bfloat16


def kernel(
    G, S, T, layers, width,
    stream, gain_pre, w_in, w_pool, pool_scale, w_out, gain_post,
    out,
    win, wout, ag, part, pair, summed, xgot, normed, acc, ss, scale, branch, ext, halo, sq,
    load_sem, zs_sem, zr_sem, ys_sem, yr_sem,
    agp_sem, agx_sem, agr_sem, ps_sem, pr_sem, xs_sem, xr_sem, qs_sem, qr_sem, hs_sem, hr_sem,
):
    g, s, t = lax.axis_index("grp"), lax.axis_index("sp"), lax.axis_index("tp")
    pairs = T // 2
    p, c = lax.div(t, 2), lax.rem(t, 2)
    mate = p * 2 + 1 - c
    R, F = stream.shape
    group = w_pool.shape[2]
    rows_in, cols_out = w_in.shape[1], w_out.shape[2]
    per = S // T
    use_y = G == 2

    def remote(src, dst, send, recv, where):
        return pltpu.make_async_remote_copy(
            src_ref=src, dst_ref=dst, send_sem=send, recv_sem=recv,
            device_id=where, device_id_type=MESH,
        )

    def span(m, src, h):
        size = rows_in if m % 2 == 0 else group
        share = size // 2 if use_y else size
        length = share // PIECES
        start = (g * share if use_y else 0) + h * length
        if m % 2 == 0:
            return win.at[m // 2, pl.ds(pl.multiple_of(src * size + start, 16), length), :]
        return wout.at[m // 2, src, pl.ds(pl.multiple_of(start, 16), length), :]

    def z_copy(m, src, way, h):
        view = span(m, src, h)
        to = s + 1 if way == 0 else s - 1
        return remote(view, view, zs_sem.at[m, src, way, h], zr_sem.at[m, src, h], {"sp": to})

    def y_copy(m, src, h):
        view = span(m, src, h)
        return remote(view, view, ys_sem.at[m, src, h], yr_sem.at[m, src, h], {"grp": 1 - g})

    def load(m):
        if m % 2 == 0:
            return pltpu.make_async_copy(
                w_in.at[m // 2],
                win.at[m // 2, pl.ds(pl.multiple_of(s * rows_in, 16), rows_in), :],
                load_sem.at[m],
            )
        return pltpu.make_async_copy(w_out.at[m // 2], wout.at[m // 2, s], load_sem.at[m])

    M = 2 * layers

    def own(m):
        if m < M:
            load(m).wait()
            for h in range(PIECES):
                pl.when(s < S - 1)(lambda: z_copy(m, s, 0, h).start())
                pl.when(s > 0)(lambda: z_copy(m, s, 1, h).start())

    def relay(m, k, h):
        def from_left():
            src = s - 1 - k
            z_copy(m, src, 0, h).wait_recv()
            pl.when(s < S - 1)(lambda: z_copy(m, src, 0, h).start())
            if use_y:
                y_copy(m, src, h).start()

        def from_right():
            src = s + 1 + k
            z_copy(m, src, 1, h).wait_recv()
            pl.when(s > 0)(lambda: z_copy(m, src, 1, h).start())
            if use_y:
                y_copy(m, src, h).start()

        pl.when(s - 1 - k >= 0)(from_left)
        pl.when(s + 1 + k <= S - 1)(from_right)

    units = [(m, k, h) for m in range(M) for k in range(S - 1) for h in range(PIECES)]
    done = [0]

    def tick(n=1):
        for mm, k, h in units[done[0] : done[0] + n]:
            relay(mm, k, h)
            if k == min(1, S - 2) and h == PIECES - 1:
                own(mm + 1)
            done[0] += 1

    def pump(m):
        tick(max(0, (m + 1) * (S - 1) * PIECES - done[0]))

    def finish(m):
        if use_y:
            for src in range(S):
                for h in range(PIECES):
                    pl.when(s != src)(lambda: y_copy(m, src, h).wait_recv())

    def cut(l):
        return R // 2 - HALO * (layers - 1) + HALO * l

    def span_in(l, a):
        return (cut(l), R) if a == 0 else (0, cut(l))

    def span_out(l, a):
        return span_in(l + 1, a)

    def bits(bounds):
        lo, hi = bounds
        mid = lo + ((hi - lo) // 2 + 15) // 16 * 16
        return [(lo, mid), (mid, hi)]

    def sweep(bounds, body):
        lo, hi = bounds
        step = 32 if (hi - lo) % 32 == 0 else 16

        def one(i, carry):
            body(pl.ds(pl.multiple_of(lo + i * step, 16), step))
            return carry

        lax.fori_loop(0, (hi - lo) // step, one, 0)

    def lanes(x):
        return sum(x[:, i : i + 128] for i in range(0, F, 128))

    def ag_copy(l, block, a, i, sem, to):
        lo, hi = bits(span_in(l, a))[i]
        view = ag.at[l, block, pl.ds(lo, hi - lo), :]
        n = a * 2 + i
        return remote(view, view, sem, agr_sem.at[l, block, n], {"tp": to})

    def ag_start(l, a):
        for i in range(2):
            n = a * 2 + i
            for d in range(1, pairs):
                q = lax.rem(p + d, pairs)
                ag_copy(l, t, a, i, agx_sem.at[l, q, n], q * 2 + c).start()
        for i in range(2):
            ag_copy(l, t, a, i, agp_sem.at[l, p, a * 2 + i], mate).start()

    def ag_wait(l, block, a):
        for i in range(2):
            ag_copy(l, block, a, i, agp_sem.at[l, p, a * 2 + i], mate).wait_recv()

    def ag_relay(l, a):
        for d in range(1, pairs):
            q = lax.rem(p + d, pairs)
            for i in range(2):
                copy = ag_copy(l, q * 2 + c, a, i, agp_sem.at[l, q, a * 2 + i], mate)
                copy.wait_recv()
                copy.start()

    def absorb(l, block, a, first):
        lo, hi = span_in(l, a)
        gain = gain_pre[pl.ds(l, 1), pl.ds(pl.multiple_of(block * F, 128), F)]

        def body(rows):
            x = ag[l, block, rows, :].astype(F32)
            square = lanes(x * x)
            ss[rows, :] = square if first else ss[rows, :] + square
            normed[rows, :] = (x * gain).astype(BF16)

        sweep((lo, hi), body)
        product = jnp.dot(
            normed[lo:hi, :], win[l, pl.ds(pl.multiple_of(block * F, 128), F), :],
            preferred_element_type=F32,
        )
        acc[lo:hi, :] = product if first else acc[lo:hi, :] + product

    def inner(l, a):
        lo, hi = span_in(l, a)
        absorb(l, t, a, True)
        ag_wait(l, mate, a)
        absorb(l, mate, a, False)
        for d in range(1, pairs):
            q = lax.rem(p + d, pairs)
            absorb(l, q * 2 + c, a, False)
            ag_wait(l, q * 2 + 1 - c, a)
            absorb(l, q * 2 + 1 - c, a, False)
        inverse = lax.rsqrt(jnp.sum(ss[lo:hi, :], axis=1, keepdims=True) / width + EPS)
        ext[l, HALO + lo : HALO + hi, :] = (acc[lo:hi, :] * inverse).astype(BF16)

    def halo_copy(l):
        return remote(
            ext.at[l, pl.ds(R, HALO), :], halo.at[l], hs_sem.at[l], hr_sem.at[l], {"sp": s + 1}
        )

    def halo_in(l):
        pl.when(s > 0)(lambda: halo_copy(l).wait_recv())

        @pl.when(s == 0)
        def _():
            ext[l, pl.ds(0, HALO), :] = jnp.zeros((HALO, group), BF16)

        @pl.when(s > 0)
        def _():
            ext[l, pl.ds(0, HALO), :] = halo[l]

    def pool(l, a):
        lo, hi = span_out(l, a)
        values = ext[l, lo : hi + HALO, :].astype(F32)
        two = values + pltpu.roll(values, 1, 0)
        four = two + pltpu.roll(two, 2, 0)
        eight = four + pltpu.roll(four, 4, 0)
        sixteen = eight + pltpu.roll(eight, 8, 0)
        total = jnp.where(t == 0, two, jnp.where(t == 1, four, jnp.where(t == 2, eight, sixteen)))
        window = jnp.where(t == 0, 2, jnp.where(t == 1, 4, jnp.where(t == 2, 8, 16)))
        place = s * R + lo + lax.broadcasted_iota(jnp.int32, (hi - lo, group), 0)
        count = jnp.minimum(place + 1, window).astype(F32)
        spread = (total[HALO:, :] / count - values[HALO:, :]).astype(BF16)
        mixed = jnp.dot(spread, w_pool[l, 0], preferred_element_type=F32)
        return (mixed * pool_scale[l : l + 1, :]).astype(BF16)

    def project(l, a, dest, mixed):
        lo, hi = span_out(l, a)
        for k in range(per):
            value = jnp.dot(mixed, wout[l, dest * per + k], preferred_element_type=F32)
            part[l, dest, lo:hi, k * cols_out : (k + 1) * cols_out] = value.astype(BF16)

    def pair_copy(l, q, a, i):
        lo, hi = bits(span_out(l, a))[i]
        rows, n = pl.ds(lo, hi - lo), a * 2 + i
        return remote(
            part.at[l, q * 2 + 1 - c, rows, :], pair.at[l, q, rows, :],
            ps_sem.at[l, q, n], pr_sem.at[l, q, n], {"tp": mate},
        )

    def cross_copy(l, q, slot, a, i):
        lo, hi = bits(span_out(l, a))[i]
        rows, n = pl.ds(lo, hi - lo), a * 2 + i
        return remote(
            summed.at[l, q, rows, :], xgot.at[l, slot, rows, :],
            xs_sem.at[l, q, n], xr_sem.at[l, slot, n], {"tp": q * 2 + c},
        )

    def scatter_first(l, a, mixed):
        for d in range(1, pairs):
            q = lax.rem(p + d, pairs)
            project(l, a, q * 2 + 1 - c, mixed)
            for i in range(2):
                pair_copy(l, q, a, i).start()
        for d in range(1, pairs):
            project(l, a, lax.rem(p + d, pairs) * 2 + c, mixed)

    def scatter_cross(l, a):
        for d in range(1, pairs):
            q = lax.rem(p + d, pairs)
            for i in range(2):
                pair_copy(l, q, a, i).wait_recv()

                def body(rows):
                    summed[l, q, rows, :] = (
                        part[l, q * 2 + c, rows, :].astype(F32) + pair[l, q, rows, :].astype(F32)
                    ).astype(BF16)

                sweep(bits(span_out(l, a))[i], body)
                cross_copy(l, q, p, a, i).start()

    def scatter_own(l, a, mixed):
        project(l, a, mate, mixed)
        for i in range(2):
            pair_copy(l, p, a, i).start()
        project(l, a, t, mixed)

    def sq_copy(l, slot, a, to):
        view = sq.at[l, a, slot]
        return remote(view, view, qs_sem.at[l, a, to], qr_sem.at[l, a, slot], {"tp": to})

    def settle(l, a):
        for i in range(2):
            pair_copy(l, p, a, i).wait_recv()
            for d in range(1, pairs):
                q = lax.rem(p + d, pairs)
                cross_copy(l, q, q, a, i).wait_recv()

            def add(rows):
                value = part[l, t, rows, :].astype(F32) + pair[l, p, rows, :].astype(F32)
                for d in range(1, pairs):
                    value = value + xgot[l, lax.rem(p + d, pairs), rows, :].astype(F32)
                branch[rows, :] = value
                ss[rows, :] = lanes(value * value)

            sweep(bits(span_out(l, a))[i], add)
        row = jnp.sum(jnp.transpose(ss[...]), axis=0, keepdims=True)
        sq[l, a, t] = jnp.broadcast_to(row, (8, R))
        for d in range(1, T):
            sq_copy(l, t, a, lax.rem(t + d, T)).start()
        tick()
        for d in range(1, T):
            other = lax.rem(t + d, T)
            sq_copy(l, other, a, other).wait_recv()
        squares = sq[l, a, 0]
        for k in range(1, T):
            squares = squares + sq[l, a, k]
        inverse = lax.rsqrt(squares / width + EPS)
        scale[...] = jnp.transpose(jnp.concatenate([inverse] * 16, axis=0))
        gain = gain_post[pl.ds(l, 1), pl.ds(pl.multiple_of(t * F, 128), F)]

        def update(rows):
            value = ag[l, t, rows, :].astype(F32) + branch[rows, :] * scale[rows, 0:1] * gain
            if l + 1 < layers:
                ag[l + 1, t, rows, :] = value.astype(BF16)
            else:
                out[rows, :] = value.astype(BF16)

        sweep(span_out(l, a), update)
        if l + 1 < layers:
            ag_start(l + 1, a)

    for m in range(M):
        load(m).start()
    barrier = pltpu.get_barrier_semaphore()

    def greet(where):
        pl.semaphore_signal(barrier, inc=1, device_id=where, device_id_type=MESH)

    pl.when(s < S - 1)(lambda: greet({"sp": s + 1}))
    pl.when(s > 0)(lambda: greet({"sp": s - 1}))
    if use_y:
        greet({"grp": 1 - g})
    for d in range(1, T):
        greet({"tp": lax.rem(t + d, T)})
    ag[0, t] = stream[...]
    ends = jnp.where(s > 0, 1, 0) + jnp.where(s < S - 1, 1, 0)
    pl.semaphore_wait(barrier, ends + (1 if use_y else 0) + T - 1)

    own(0)
    ag_start(0, 0)
    ag_start(0, 1)
    each = (S - 1) * PIECES
    for l in range(layers):
        if l == 0:
            tick(each // 3)
            ag_relay(0, 0)
            tick(each // 3)
            ag_relay(0, 1)
        else:
            ag_relay(l, 0)
        pump(2 * l)
        finish(2 * l)
        inner(l, 0)
        pl.when(s < S - 1)(lambda: halo_copy(l).start())
        mixed = pool(l, 0)
        if l == 0:
            tick()
            inner(l, 1)
            tick()
            halo_in(l)
            later = pool(l, 1)
        pump(2 * l + 1)
        finish(2 * l + 1)
        scatter_first(l, 0, mixed)
        tick()
        if l > 0:
            ag_relay(l, 1)
        scatter_cross(l, 0)
        tick()
        scatter_own(l, 0, mixed)
        tick()
        if l > 0:
            inner(l, 1)
            tick()
            halo_in(l)
            later = pool(l, 1)
        scatter_first(l, 1, later)
        tick()
        scatter_cross(l, 1)
        tick()
        scatter_own(l, 1, later)
        tick()
        settle(l, 0)
        tick()
        settle(l, 1)
        tick()

    for l in range(layers):
        pl.when(s < S - 1)(lambda: halo_copy(l).wait_send())
        for a in range(2):
            for d in range(1, T):
                sq_copy(l, t, a, lax.rem(t + d, T)).wait_send()
            for i in range(2):
                n = a * 2 + i
                for q in range(pairs):
                    ag_copy(l, t, a, i, agp_sem.at[l, q, n], mate).wait_send()
                    pair_copy(l, q, a, i).wait_send()
                for d in range(1, pairs):
                    q = lax.rem(p + d, pairs)
                    ag_copy(l, t, a, i, agx_sem.at[l, q, n], mate).wait_send()
                    cross_copy(l, q, p, a, i).wait_send()
    for m in range(M):
        for src in range(S):
            for h in range(PIECES):
                pl.when(jnp.logical_and(src <= s, s < S - 1))(lambda: z_copy(m, src, 0, h).wait_send())
                pl.when(jnp.logical_and(src >= s, s > 0))(lambda: z_copy(m, src, 1, h).wait_send())
                if use_y:
                    pl.when(s != src)(lambda: y_copy(m, src, h).wait_send())


def per_device(G, S, T, stream, gain_pre, w_in, w_pool, pool_scale, w_out, gain_post):
    layers, width = gain_pre.shape
    R, F = stream.shape
    group = w_pool.shape[2]
    pairs = T // 2
    M = 2 * layers
    dma = pltpu.SemaphoreType.DMA
    vmem = pl.BlockSpec(memory_space=pltpu.VMEM)
    anywhere = pl.BlockSpec(memory_space=pl.ANY)
    return pl.pallas_call(
        functools.partial(kernel, G, S, T, layers, width),
        out_shape=jax.ShapeDtypeStruct((R, F), BF16),
        in_specs=[vmem, vmem, anywhere, vmem, vmem, anywhere, vmem],
        out_specs=vmem,
        scratch_shapes=[
            pltpu.VMEM((layers, width, group), BF16),
            pltpu.VMEM((layers, S, group, w_out.shape[2]), BF16),
            pltpu.VMEM((layers, T, R, F), BF16),
            pltpu.VMEM((layers, T, R, F), BF16),
            pltpu.VMEM((layers, pairs, R, F), BF16),
            pltpu.VMEM((layers, pairs, R, F), BF16),
            pltpu.VMEM((layers, pairs, R, F), BF16),
            pltpu.VMEM((R, F), BF16),
            pltpu.VMEM((R, group), F32),
            pltpu.VMEM((R, 128), F32),
            pltpu.VMEM((R, 128), F32),
            pltpu.VMEM((R, F), F32),
            pltpu.VMEM((layers, HALO + R, group), BF16),
            pltpu.VMEM((layers, HALO, group), BF16),
            pltpu.VMEM((layers, 2, T, 8, R), F32),
            dma((M,)),
            dma((M, S, 2, PIECES)),
            dma((M, S, PIECES)),
            dma((M, S, PIECES)),
            dma((M, S, PIECES)),
            dma((layers, pairs, CHUNKS)),
            dma((layers, pairs, CHUNKS)),
            dma((layers, T, CHUNKS)),
            dma((layers, pairs, CHUNKS)),
            dma((layers, pairs, CHUNKS)),
            dma((layers, pairs, CHUNKS)),
            dma((layers, pairs, CHUNKS)),
            dma((layers, 2, T)),
            dma((layers, 2, T)),
            dma((layers,)),
            dma((layers,)),
        ],
        compiler_params=pltpu.CompilerParams(
            collective_id=0, has_side_effects=True, vmem_limit_bytes=60 * 1024 * 1024
        ),
    )(stream, gain_pre, w_in, w_pool, pool_scale, w_out, gain_post)


def plane_kernel(
    G, S, T, layers, width, order,
    stream_hbm, gain_pre_hbm, w_in, w_pool, scale_hbm, w_out, gain_post_hbm,
    out,
    stream, gain_pre, gain_post, win, wout, wp, scales, rows_in, x, held,
    part, got, far, edge, psq, esq, mix, branch, bsq,
    load_sem, small_sem, self_sem, y_send, y_recv, x_send, x_recv, f_send, f_recv,
    wo_send, wo_recv, wx_send, wx_recv, wy_send, wy_recv, wf_send, wf_recv,
    p_send, p_recv, c_send, c_recv,
    r_send, r_recv, o_send, o_recv, rq_send, rq_recv, h_send, h_recv, hq_send, hq_recv, m_send, m_recv, mq_send, mq_recv,
):
    g, s, t = lax.axis_index("grp"), lax.axis_index("sp"), lax.axis_index("tp")
    pairs = T // 2
    p, c = lax.div(t, 2), lax.rem(t, 2)
    mate = p * 2 + 1 - c
    R, F = stream.shape
    C = R // T
    group = w_pool.shape[2]
    sides = 2 if G == 2 else 1
    side = g if sides == 2 else 0
    M = 2 * layers
    line_width = psq.shape[-1]
    H = S // 2
    low = lax.div(s, H) * H
    here = s - low
    hub, far_hub = jnp.where(low == 0, H - 1, H), jnp.where(low == 0, H, H - 1)
    is_hub = s == hub
    near = [low + lax.rem(here + d, H) for d in range(1, H)]
    away = [H - low + d for d in range(H)]
    planes = near + away

    def slot(k):
        return lax.rem(k - low + S, S)

    def remote(src, dst, send, recv, where):
        return pltpu.make_async_remote_copy(
            src_ref=src, dst_ref=dst, send_sem=send, recv_sem=recv,
            device_id=where, device_id_type=MESH,
        )

    def sent(view, sem):
        remote(view, view, sem, sem, {"tp": mate}).wait_send()

    def landed(view, sem):
        remote(view, view, sem, sem, {"tp": mate}).wait_recv()

    barrier = pltpu.get_barrier_semaphore()

    def greet(where):
        pl.semaphore_signal(barrier, inc=1, device_id=where, device_id_type=MESH)

    for ds in range(S):
        for dt in range(T):
            if ds or dt:
                greet({"sp": lax.rem(s + ds, S), "tp": lax.rem(t + dt, T)})
    if sides == 2:
        greet({"grp": 1 - g})

    smalls = [
        pltpu.make_async_copy(stream_hbm, stream, small_sem.at[0]),
        pltpu.make_async_copy(gain_pre_hbm, gain_pre, small_sem.at[1]),
        pltpu.make_async_copy(gain_post_hbm, gain_post, small_sem.at[2]),
    ]
    scale_load = pltpu.make_async_copy(scale_hbm, scales, small_sem.at[3])

    def block(m, k):
        if m % 2 == 0:
            return win.at[m // 2, slot(k)]
        return wout.at[m // 2, pl.ds(pl.multiple_of(slot(k) * group, 16), group), :]

    def piece(m, k, half, h):
        rows = (F if m % 2 == 0 else group) // sides
        length = rows // PARTS
        start = half * rows + h * length
        if m % 2 == 0:
            return win.at[m // 2, slot(k), pl.ds(pl.multiple_of(start, 16), length), :]
        return wout.at[m // 2, pl.ds(pl.multiple_of(slot(k) * group + start, 16), length), :]

    def load(m):
        return pltpu.make_async_copy((w_out if m % 2 else w_in).at[m // 2], block(m, t), load_sem.at[m])

    def own_copy(m, k):
        return remote(block(m, k), block(m, k), wo_send.at[m], wo_recv.at[m], {"tp": mate})

    def cross_copy(m, k, d, q, h):
        view = piece(m, k, side, h)
        return remote(view, view, wx_send.at[m, d], wx_recv.at[m, d, h], {"tp": q * 2 + c})

    def grp_copy(m, d, q, half, h):
        view = piece(m, q * 2 + c, half, h)
        return remote(view, view, wy_send.at[m, d], wy_recv.at[m, d, h], {"grp": 1 - g})

    def mate_copy(m, d, q, half, h):
        view = piece(m, q * 2 + c, half, h)
        return remote(view, view, wf_send.at[m, d], wf_recv.at[m, d], {"tp": mate})

    others = [(d, lax.rem(p + 1 + d, pairs)) for d in range(pairs - 1)]

    def weight_own(m):
        load(m).wait()
        own_copy(m, t).start()

    def weight_cross(m, h):
        for d, q in others:
            back = pairs - 2 - d
            view = piece(m, t, side, h)
            remote(view, view, wx_send.at[m, d], wx_recv.at[m, back, h], {"tp": q * 2 + c}).start()

    def weight_relay(m, h):
        for d, q in others:
            cross_copy(m, q * 2 + c, d, q, h).wait_recv()
            if sides == 2:
                grp_copy(m, d, q, side, h).start()
            mate_copy(m, d, q, side, h).start()

    def weight_second(m, h):
        if sides == 2:
            for d, q in others:
                grp_copy(m, d, q, 1 - side, h).wait_recv()
                mate_copy(m, d, q, 1 - side, h).start()

    def weight_last(m):
        for d, q in others:
            landed(block(m, q * 2 + 1 - c), wf_recv.at[m, d])

    def share(m, k):
        rows = (F if m % 2 == 0 else group) // sides
        if m % 2 == 0:
            return win.at[m // 2, slot(k), pl.ds(0, rows), :]
        return wout.at[m // 2, pl.ds(pl.multiple_of(slot(k) * group, 16), rows), :]

    def pool_copy(l, d):
        return remote(wp.at[l], wp.at[l], p_send.at[d - 1], p_recv.at[l], {"tp": lax.rem(t + d, T)})

    def scale_copy(d):
        return remote(scales, scales, c_send.at[d - 1], c_recv, {"tp": lax.rem(t + d, T)})

    def pool_send(l):
        @pl.when(t == s)
        def _():
            for d in range(1, T):
                pool_copy(l, d).start()

    def lanes(v):
        return sum(v[:, i : i + 128] for i in range(0, F, 128))

    def line(square):
        if C < line_width:
            square = jnp.concatenate([square, jnp.zeros((line_width - C, 128), F32)], axis=0)
        row = jnp.sum(jnp.transpose(square), axis=0, keepdims=True)
        return jnp.broadcast_to(row, (8, line_width))

    def column(values, first=0):
        return jnp.transpose(jnp.concatenate([values] * 16, axis=0))[first:C]

    def wide(values, n):
        return jnp.concatenate([values] * (n // 128), axis=1)

    def squares_start(ref, l, q, send, recv):
        for d in range(1, S):
            remote(ref.at[l, q, 0], ref.at[l, q, d], send, recv.at[q], {"sp": lax.rem(s + d, S)}).start()

    def squares_wait(ref, l, q, recv):
        landed(ref.at[l, q, pl.ds(1, S - 1)], recv.at[q])

    def total(ref, l, q):
        return sum(ref[l, q, k] for k in range(S))

    def next_run(l, q, start):
        if q + 1 < S:
            start(q + lax.div(t + 1, T), 0)
        else:
            pl.when(t + 1 < T)(lambda: start(q, 1))

    def edge_copy(l, q, k, index, plane, final):
        def start(ahead, last):
            remote(
                part.at[l, q, k, pl.ds(C - HALO, HALO), :], edge.at[l, ahead, index],
                h_send.at[2 * final + last], h_recv.at[l, ahead], {"sp": plane, "tp": lax.rem(t + 1, T)},
            ).start()

        next_run(l, q, start)

    def edge_squares(l, q):
        def start(ahead, last):
            for d in range(S):
                remote(
                    psq.at[l, q, 0], esq.at[l, ahead, d], hq_send.at[last], hq_recv.at[l, ahead],
                    {"sp": lax.rem(s + d, S), "tp": lax.rem(t + 1, T)},
                ).start()

        next_run(l, q, start)

    def run_copy(to, origin):
        rows = pl.ds(pl.multiple_of(to * C, 16), C)
        return remote(stream.at[rows, :], rows_in.at[origin], y_send, y_recv.at[origin], {"tp": to})

    def run_of(f, local):
        return stream.at[pl.ds(pl.multiple_of(t * C, 16), C), :] if local else rows_in.at[f]

    def stream_self(local):
        return pltpu.make_async_copy(run_of(s, local), x.at[s], self_sem.at[0])

    def stream_on(f, local=False):
        pl.when(f == s)(lambda: stream_self(local).start())
        pl.when(f != s)(
            lambda: remote(run_of(f, local), x.at[s], x_send, x_recv.at[s], {"sp": f}).start()
        )

    def final_copy(q):
        rows = pl.ds(pl.multiple_of(t * C, 16), C)
        return remote(x.at[q], out.at[rows, :], f_send, f_recv, {"sp": q, "tp": s})

    def final_self(q):
        rows = pl.ds(pl.multiple_of(t * C, 16), C)
        return pltpu.make_async_copy(x.at[q], out.at[rows, :], self_sem.at[1])

    def features(ref, l):
        return ref[pl.ds(l, 1), pl.ds(pl.multiple_of(s * F, 128), F)]

    def stage_a(l, q):
        with jax.named_scope(f"a{l}{q}"):
            advance(l, q)

    def advance(l, q):
        if l == 0:
            pl.when(s == q)(lambda: stream_self(False).wait())
            pl.when(s != q)(lambda: landed(x.at[q], x_recv.at[q]))
            value = x[q].astype(F32)
        else:
            squares_wait(bsq, l - 1, q, mq_recv)
            inverse = column(lax.rsqrt(total(bsq, l - 1, q) / width + EPS))
            new = x[q].astype(F32) + branch[q] * wide(inverse, F) * features(gain_post, l - 1)
            new = new.astype(BF16)
            x[q] = new
            if l == layers:
                return
            value = new.astype(F32)
        scaled = (value * features(gain_pre, l)).astype(BF16)
        if l == 0:
            held[q] = scaled
            pl.when(p == low // H)(lambda: inward(l, q, scaled))
            pl.when(p != low // H)(lambda: outward(l, q, scaled))
        else:
            if q == 0:
                ready(2 * l)
            outward(l, q, scaled)
        psq[l, q, 0] = line(lanes(value * value))
        squares_start(psq, l, q, rq_send, rq_recv)
        edge_squares(l, q)
        if l > 0:
            inward(l, q, scaled)

    def stage_e(q):
        with jax.named_scope(f"e{q}"):
            pl.when(p == low // H)(lambda: outward(0, q, held[q]))
            pl.when(p != low // H)(lambda: inward(0, q, held[q]))

    def weight_first():
        with jax.named_scope("first"):
            weight_last(0)

    def stage_z(q):
        mine = jnp.logical_and(s == q, t == s)
        pl.when(mine)(lambda: final_self(q).start())
        pl.when(jnp.logical_not(mine))(lambda: final_copy(q).start())

    def project(l, q, k, scaled):
        part[l, q, k] = jnp.dot(scaled, win[l, k], preferred_element_type=F32).astype(BF16)

    def outward(l, q, scaled):
        for k in range(H, S):
            project(l, q, k, scaled)

        @pl.when(jnp.logical_not(is_hub))
        def _():
            index = jnp.where(here > hub - low, here - 1, here)
            remote(
                part.at[l, q, pl.ds(H, H)], far.at[l, q, index], o_send, o_recv.at[q], {"sp": hub}
            ).start()

    def inward(l, q, scaled):
        for k in range(H):
            project(l, q, k, scaled)
        for d, k in enumerate(near):
            remote(
                part.at[l, q, slot(k)], got.at[l, q, H - 2 - d], r_send, r_recv.at[q], {"sp": k}
            ).start()
            edge_copy(l, q, slot(k), H - 2 - d, k, 0)
        edge_copy(l, q, here, H, s, 0)

    def stage_s(l, q):
        with jax.named_scope(f"s{l}{q}"):

            @pl.when(is_hub)
            def _():
                landed(far.at[l, q], o_recv.at[q])
                for k in range(H):
                    value = part[l, q, H + k].astype(F32)
                    for d in range(H - 1):
                        value = value + far[l, q, d, k].astype(F32)
                    part[l, q, H + k] = value.astype(BF16)
                    remote(
                        part.at[l, q, H + k], got.at[l, q, H - 1], o_send, r_recv.at[q], {"sp": away[k]}
                    ).start()
                    edge_copy(l, q, H + k, H - 1, away[k], 1)

    def ready(m):
        landed(block(m, mate), wo_recv.at[m])
        weight_last(m)

    def stage_b(l, q):
        with jax.named_scope(f"b{l}{q}"):
            smooth(l, q)

    def smooth(l, q):
        squares_wait(psq, l, q, rq_recv)
        inverse = column(lax.rsqrt(total(psq, l, q) / width + EPS))

        def arrived():
            landed(esq.at[l, q], hq_recv.at[l, q])
            landed(edge.at[l, q], h_recv.at[l, q])

        if q == 0:
            pl.when(t > 0)(arrived)
            pl.when(t != s)(lambda: landed(wp.at[l], p_recv.at[l]))
            if l == 0:
                pl.when(t != s)(lambda: landed(scales, c_recv))
        else:
            arrived()
        before = column(lax.rsqrt(total(esq, l, q) / width + EPS), C - HALO)
        ahead = sum(edge[l, q, k].astype(F32) for k in range(H + 1))
        landed(got.at[l, q], r_recv.at[q])
        value = part[l, q, here].astype(F32)
        for k in range(H):
            value = value + got[l, q, k].astype(F32)
        values = jnp.concatenate([ahead * wide(before, group), value * wide(inverse, group)], axis=0)
        values = values.astype(BF16).astype(F32)
        reach = values
        pooled = values
        for k in range(S):
            reach = reach + pltpu.roll(reach, 2**k, 0)
            pooled = jnp.where(s == k, reach, pooled)
        window = jnp.left_shift(2, s)
        place = q * R + t * C + lax.broadcasted_iota(jnp.int32, (C, group), 0)
        count = jnp.minimum(place + 1, window).astype(F32)
        spread = (pooled[HALO:, :] / count - values[HALO:, :]).astype(BF16)
        mixed = jnp.dot(spread, wp[l], preferred_element_type=F32)
        mix[l, q, here] = (mixed * scales[l : l + 1, :]).astype(BF16)

        def on(k, kind):
            lower = lax.div(k, H) * H
            remote(
                mix.at[l, q, here], mix.at[l, q, lax.rem(s - lower + S, S)],
                m_send.at[3 if kind else 0], m_recv.at[kind, q], {"sp": k},
            ).start()

        for k in near if RELAYED else planes:
            on(k, 0)
        if RELAYED:
            pl.when(is_hub)(lambda: on(far_hub, 1))

    def mates_view(l, q):
        return mix.at[l, q, pl.ds(0, H - 1)]

    def stage_f(l, q):
        with jax.named_scope(f"f{l}{q}"):

            @pl.when(is_hub)
            def _():
                landed(mates_view(l, q), m_recv.at[0, q])
                for j in range(1, H):
                    from_here = lax.rem(here + j, H)
                    for k in away:
                        remote(
                            mix.at[l, q, from_here], mix.at[l, q, H + from_here],
                            m_send.at[1], m_recv.at[2, q], {"sp": k},
                        ).start()

    def stage_g(l, q):
        with jax.named_scope(f"g{l}{q}"):

            @pl.when(is_hub)
            def _():
                spot = slot(far_hub)
                landed(mix.at[l, q, spot], m_recv.at[1, q])
                for k in near:
                    remote(
                        mix.at[l, q, spot], mix.at[l, q, spot],
                        m_send.at[2], m_recv.at[1, q], {"sp": k},
                    ).start()

    def stage_d(l, q):
        with jax.named_scope(f"d{l}{q}"):
            if q == 0:
                ready(2 * l + 1)

            if RELAYED:

                @pl.when(jnp.logical_not(is_hub))
                def _():
                    landed(mates_view(l, q), m_recv.at[0, q])
                    landed(mix.at[l, q, 0], m_recv.at[1, q])

                landed(mates_view(l, q), m_recv.at[2, q])
            else:
                landed(mix.at[l, q, pl.ds(0, S - 1)], m_recv.at[0, q])
            value = jnp.dot(
                jnp.concatenate([mix[l, q, k] for k in range(S)], axis=1), wout[l],
                preferred_element_type=F32,
            )
            branch[q] = value
            bsq[l, q, 0] = line(lanes(value * value))
            squares_start(bsq, l, q, mq_send, mq_recv)

    smalls[0].start()
    for m in range(M):
        load(m).start()
    smalls[1].start()
    smalls[2].start()
    pool_load = [pltpu.make_async_copy(w_pool.at[l, 0], wp.at[l], p_recv.at[l]) for l in range(layers)]

    @pl.when(t == s)
    def _():
        for l in range(layers):
            pool_load[l].start()
        scale_load.start()

    @pl.when(t == 0)
    def _():
        for l in range(layers):
            edge[l, 0] = jnp.zeros(edge.shape[2:], BF16)
            esq[l, 0] = jnp.zeros(esq.shape[2:], F32)

    smalls[0].wait()
    pl.semaphore_wait(barrier, S * T - 1 + (1 if sides == 2 else 0))

    for _, q in others:
        run_copy(q * 2 + c, t).start()
        run_copy(q * 2 + 1 - c, t).start()
    run_copy(mate, t).start()
    stream_on(t, True)
    weight_own(0)
    for h in range(PARTS):
        weight_cross(0, h)
    weight_own(1)
    for h in range(PARTS):
        weight_cross(1, h)
    with jax.named_scope("enter"):
        landed(rows_in.at[mate], y_recv.at[mate])
        stream_on(mate)
        for _, q in others:
            for core in (c, 1 - c):
                landed(rows_in.at[q * 2 + core], y_recv.at[q * 2 + core])
                stream_on(q * 2 + core)
        for h in range(PARTS):
            weight_relay(0, h)
    landed(block(0, mate), wo_recv.at[0])

    @pl.when(t == s)
    def _():
        for l in range(layers):
            pool_load[l].wait()
        scale_load.wait()
        for d in range(1, T):
            scale_copy(d).start()

    pool_send(0)
    smalls[1].wait()
    smalls[2].wait()

    actions = (
        stage_a, stage_b, None, stage_d, weight_own, pool_send, weight_cross, weight_relay, weight_second,
        stage_s, stage_f, stage_g, stage_z, stage_e, weight_first,
    )
    for kind, *where in order:
        actions[kind](*where)

    rows = pl.ds(0, (T - 1) * C)

    @pl.when(s == t)
    def _():
        final_self(s).wait()
        landed(out.at[rows, :], f_recv)
        sent(out.at[rows, :], f_send)

    @pl.when(s != t)
    def _():
        landed(out, f_recv)
        sent(out, f_send)

    with jax.named_scope("drain"):
        sent(stream.at[rows, :], y_send)
        sent(x.at[pl.ds(0, S - 1)], x_send)

        @pl.when(t == s)
        def _():
            for d in range(1, T):
                sent(scales, c_send.at[d - 1])
                sent(wp, p_send.at[d - 1])

        for m in range(M):
            sent(block(m, t), wo_send.at[m])
            for d, q in others:
                sent(share(m, t), wx_send.at[m, d])
                sent(block(m, t), wf_send.at[m, d])
                if sides == 2:
                    sent(share(m, t), wy_send.at[m, d])
        sent(psq.at[:, :, pl.ds(0, S - 1)], rq_send)
        sent(bsq.at[:, :, pl.ds(0, S - 1)], mq_send)
        sent(part.at[:, :, pl.ds(0, H - 1)], r_send)
        sent(part.at[:, :, pl.ds(0, H)], o_send)
        sent(mix.at[:, :, pl.ds(0, (H if RELAYED else S) - 1)], m_send.at[0])

        @pl.when(is_hub if RELAYED else s < 0)
        def _():
            sent(mix.at[:, :, 0], m_send.at[3])
            sent(mix.at[:, :, pl.ds(0, (H - 1) * H)], m_send.at[1])
            sent(mix.at[:, :, pl.ds(0, H - 1)], m_send.at[2])

        sent(edge.at[:, pl.ds(0, S - 1), pl.ds(0, H)], h_send.at[0])
        sent(esq.at[:, pl.ds(0, S - 1)], hq_send.at[0])
        pl.when(is_hub)(lambda: sent(edge.at[:, pl.ds(0, S - 1), pl.ds(0, H)], h_send.at[2]))

        @pl.when(t + 1 < T)
        def _():
            sent(edge.at[:, 0, pl.ds(0, H)], h_send.at[1])
            sent(esq.at[:, 0], hq_send.at[1])
            pl.when(is_hub)(lambda: sent(edge.at[:, 0, pl.ds(0, H)], h_send.at[3]))


def stage_order(layers, runs):
    steps = []
    begins = {0: 0, 9: AT_S, 1: AT_B, 3: AT_D}
    if RELAYED:
        begins |= {10: AT_F, 11: AT_G}
    steps.append((-90, (14,)))
    for h in range(PARTS):
        steps.append((-100 + EARLY[0] + h * EARLY[1], (8, 0, h)))
    for l in range(layers + 1):
        for kind, at in begins.items():
            if l < layers or kind == 0:
                for q in range(runs):
                    pace = STRIDES[0 if l == 0 else 1 if l + 1 < layers else 2]
                    if l == 0 and kind == 0:
                        steps.append((q - 100, (0, 0, q)))
                        steps.append((q * pace, (13, q)))
                    else:
                        steps.append((l * PERIOD + at + q * pace, (kind, l, q)))
    last = max(at for at, step in steps if step[0] == 3)
    for at, step in list(steps):
        if step[:2] == (0, layers):
            steps.append((max(at, last + AT_Z) + 0.01, (12, step[2])))
    for m in range(1, 2 * layers):
        due = m // 2 * PERIOD + (AT_D if m % 2 else 0) - 0.1
        odd = m % 2
        begin = due - LEADS[odd]
        relay, second = RELAYS[odd], SECONDS[odd]
        if m == 1:
            relay, second = FIRST
            begin = due - (PARTS - 1) * SPACE - relay - second
        for h in range(PARTS):
            if m > 1:
                if h == 0:
                    steps.append((begin, (4, m)))
                    if m % 2 == 0:
                        steps.append((begin, (5, m // 2)))
                steps.append((begin + h * SPACE, (6, m, h)))
            steps.append((begin + h * SPACE + relay, (7, m, h)))
            steps.append((begin + h * SPACE + relay + second, (8, m, h)))
    return [step for _, step in sorted(steps)]


def per_plane(G, S, T, stream, gain_pre, w_in, w_pool, pool_scale, w_out, gain_post):
    layers, width = gain_pre.shape
    R, F = stream.shape
    group = w_pool.shape[2]
    C = R // T
    H = S // 2
    pairs = T // 2
    M = 2 * layers
    wide = max(128, C)
    dma = pltpu.SemaphoreType.DMA
    anywhere = pl.BlockSpec(memory_space=pl.ANY)
    return pl.pallas_call(
        functools.partial(plane_kernel, G, S, T, layers, width, stage_order(layers, S)),
        out_shape=jax.ShapeDtypeStruct((R, F), BF16),
        in_specs=[anywhere] * 7,
        out_specs=OUT_SPEC,
        scratch_shapes=[
            pltpu.VMEM((R, F), BF16),
            pltpu.VMEM((layers, width), F32),
            pltpu.VMEM((layers, width), F32),
            pltpu.VMEM((layers, T, F, group), BF16),
            pltpu.VMEM((layers, T * group, F), BF16),
            pltpu.VMEM((layers, group, group), BF16),
            pltpu.VMEM((layers, group), F32),
            pltpu.VMEM((T, C, F), BF16),
            pltpu.VMEM((S, C, F), BF16),
            pltpu.VMEM((S, C, F), BF16),
            pltpu.VMEM((layers, S, S, C, group), BF16),
            pltpu.VMEM((layers, S, H, C, group), BF16),
            pltpu.VMEM((layers, S, H - 1, H, C, group), BF16),
            pltpu.VMEM((layers, S, H + 1, HALO, group), BF16),
            pltpu.VMEM((layers, S, S, 8, wide), F32),
            pltpu.VMEM((layers, S, S, 8, wide), F32),
            pltpu.VMEM((layers, S, S, C, group), BF16),
            pltpu.VMEM((S, C, F), F32),
            pltpu.VMEM((layers, S, S, 8, wide), F32),
            dma((M,)),
            dma((4,)),
            dma((2,)),
            dma(()),
            dma((T,)),
            dma(()),
            dma((S,)),
            dma(()),
            dma(()),
            dma((M,)),
            dma((M,)),
            dma((M, pairs - 1)),
            dma((M, pairs - 1, PARTS)),
            dma((M, pairs - 1)),
            dma((M, pairs - 1, PARTS)),
            dma((M, pairs - 1)),
            dma((M, pairs - 1)),
            dma((T - 1,)),
            dma((layers,)),
            dma((T - 1,)),
            dma(()),
            dma(()),
            dma((S,)),
            dma(()),
            dma((S,)),
            dma(()),
            dma((S,)),
            dma((4,)),
            dma((layers, S)),
            dma((2,)),
            dma((layers, S)),
            dma((4,)),
            dma((3, S)),
            dma(()),
            dma((S,)),
        ],
        compiler_params=pltpu.CompilerParams(
            collective_id=0, has_side_effects=True, vmem_limit_bytes=60 * 1024 * 1024
        ),
    )(stream, gain_pre, w_in, w_pool, pool_scale, w_out, gain_post)


def plan(G, S, T, *args):
    stream, w_pool = args[0], args[3]
    planes = S == T == T * w_pool.shape[1] and S // 2 == T // 2 == 2 and stream.shape[0] % (HALO * T) == 0
    return (per_plane if planes else per_device)(G, S, T, *args)


def solution(mesh):
    G, S, T = mesh.shape["grp"], mesh.shape["sp"], mesh.shape["tp"]
    return jax.shard_map(
        functools.partial(plan, G, S, T),
        mesh=mesh,
        in_specs=(
            P(("grp", "sp"), "tp"),
            P(),
            P(None, "sp", "tp"),
            P(None, "tp", None, None),
            P(None, "tp"),
            P(None, "tp", "sp"),
            P(),
        ),
        out_specs=P(("grp", "sp"), "tp"),
        check_vma=False,
    )
```

```python
import functools

import jax
import jax.numpy as jnp
from jax import lax
from jax.experimental import pallas as pl
from jax.experimental.pallas import tpu as pltpu
from jax.sharding import PartitionSpec as P

EPS = 1e-06
HALO = 16
CHUNKS = 4
PIECES = 2
PARTS = 4
RELAYED = True
OUT_SPEC = pl.BlockSpec(memory_space=pl.ANY)
PERIOD, STRIDES = 17, (2, 2.5, 2.5)
AT_S, AT_B, AT_F, AT_G, AT_D, AT_Z = 2.3, 5.6, 9.6, 9.7, 13, 0
CUTS = 2
EARLY = (1.5, 0.75)
SPACE, LEADS, RELAYS, SECONDS, FIRST = 1.3, (16.9, 16.9), (9, 8), (3.4, 4), (8, 4)
MESH = pl.DeviceIdType.MESH
F32 = jnp.float32
BF16 = jnp.bfloat16


def kernel(
    G, S, T, layers, width,
    stream, gain_pre, w_in, w_pool, pool_scale, w_out, gain_post,
    out,
    win, wout, ag, part, pair, summed, xgot, normed, acc, ss, scale, branch, ext, halo, sq,
    load_sem, zs_sem, zr_sem, ys_sem, yr_sem,
    agp_sem, agx_sem, agr_sem, ps_sem, pr_sem, xs_sem, xr_sem, qs_sem, qr_sem, hs_sem, hr_sem,
):
    g, s, t = lax.axis_index("grp"), lax.axis_index("sp"), lax.axis_index("tp")
    pairs = T // 2
    p, c = lax.div(t, 2), lax.rem(t, 2)
    mate = p * 2 + 1 - c
    R, F = stream.shape
    group = w_pool.shape[2]
    rows_in, cols_out = w_in.shape[1], w_out.shape[2]
    per = S // T
    use_y = G == 2

    def remote(src, dst, send, recv, where):
        return pltpu.make_async_remote_copy(
            src_ref=src, dst_ref=dst, send_sem=send, recv_sem=recv,
            device_id=where, device_id_type=MESH,
        )

    def span(m, src, h):
        size = rows_in if m % 2 == 0 else group
        share = size // 2 if use_y else size
        length = share // PIECES
        start = (g * share if use_y else 0) + h * length
        if m % 2 == 0:
            return win.at[m // 2, pl.ds(pl.multiple_of(src * size + start, 16), length), :]
        return wout.at[m // 2, src, pl.ds(pl.multiple_of(start, 16), length), :]

    def z_copy(m, src, way, h):
        view = span(m, src, h)
        to = s + 1 if way == 0 else s - 1
        return remote(view, view, zs_sem.at[m, src, way, h], zr_sem.at[m, src, h], {"sp": to})

    def y_copy(m, src, h):
        view = span(m, src, h)
        return remote(view, view, ys_sem.at[m, src, h], yr_sem.at[m, src, h], {"grp": 1 - g})

    def load(m):
        if m % 2 == 0:
            return pltpu.make_async_copy(
                w_in.at[m // 2],
                win.at[m // 2, pl.ds(pl.multiple_of(s * rows_in, 16), rows_in), :],
                load_sem.at[m],
            )
        return pltpu.make_async_copy(w_out.at[m // 2], wout.at[m // 2, s], load_sem.at[m])

    M = 2 * layers

    def own(m):
        if m < M:
            load(m).wait()
            for h in range(PIECES):
                pl.when(s < S - 1)(lambda: z_copy(m, s, 0, h).start())
                pl.when(s > 0)(lambda: z_copy(m, s, 1, h).start())

    def relay(m, k, h):
        def from_left():
            src = s - 1 - k
            z_copy(m, src, 0, h).wait_recv()
            pl.when(s < S - 1)(lambda: z_copy(m, src, 0, h).start())
            if use_y:
                y_copy(m, src, h).start()

        def from_right():
            src = s + 1 + k
            z_copy(m, src, 1, h).wait_recv()
            pl.when(s > 0)(lambda: z_copy(m, src, 1, h).start())
            if use_y:
                y_copy(m, src, h).start()

        pl.when(s - 1 - k >= 0)(from_left)
        pl.when(s + 1 + k <= S - 1)(from_right)

    units = [(m, k, h) for m in range(M) for k in range(S - 1) for h in range(PIECES)]
    done = [0]

    def tick(n=1):
        for mm, k, h in units[done[0] : done[0] + n]:
            relay(mm, k, h)
            if k == min(1, S - 2) and h == PIECES - 1:
                own(mm + 1)
            done[0] += 1

    def pump(m):
        tick(max(0, (m + 1) * (S - 1) * PIECES - done[0]))

    def finish(m):
        if use_y:
            for src in range(S):
                for h in range(PIECES):
                    pl.when(s != src)(lambda: y_copy(m, src, h).wait_recv())

    def cut(l):
        return R // 2 - HALO * (layers - 1) + HALO * l

    def span_in(l, a):
        return (cut(l), R) if a == 0 else (0, cut(l))

    def span_out(l, a):
        return span_in(l + 1, a)

    def bits(bounds):
        lo, hi = bounds
        mid = lo + ((hi - lo) // 2 + 15) // 16 * 16
        return [(lo, mid), (mid, hi)]

    def sweep(bounds, body):
        lo, hi = bounds
        step = 32 if (hi - lo) % 32 == 0 else 16

        def one(i, carry):
            body(pl.ds(pl.multiple_of(lo + i * step, 16), step))
            return carry

        lax.fori_loop(0, (hi - lo) // step, one, 0)

    def lanes(x):
        return sum(x[:, i : i + 128] for i in range(0, F, 128))

    def ag_copy(l, block, a, i, sem, to):
        lo, hi = bits(span_in(l, a))[i]
        view = ag.at[l, block, pl.ds(lo, hi - lo), :]
        n = a * 2 + i
        return remote(view, view, sem, agr_sem.at[l, block, n], {"tp": to})

    def ag_start(l, a):
        for i in range(2):
            n = a * 2 + i
            for d in range(1, pairs):
                q = lax.rem(p + d, pairs)
                ag_copy(l, t, a, i, agx_sem.at[l, q, n], q * 2 + c).start()
        for i in range(2):
            ag_copy(l, t, a, i, agp_sem.at[l, p, a * 2 + i], mate).start()

    def ag_wait(l, block, a):
        for i in range(2):
            ag_copy(l, block, a, i, agp_sem.at[l, p, a * 2 + i], mate).wait_recv()

    def ag_relay(l, a):
        for d in range(1, pairs):
            q = lax.rem(p + d, pairs)
            for i in range(2):
                copy = ag_copy(l, q * 2 + c, a, i, agp_sem.at[l, q, a * 2 + i], mate)
                copy.wait_recv()
                copy.start()

    def absorb(l, block, a, first):
        lo, hi = span_in(l, a)
        gain = gain_pre[pl.ds(l, 1), pl.ds(pl.multiple_of(block * F, 128), F)]

        def body(rows):
            x = ag[l, block, rows, :].astype(F32)
            square = lanes(x * x)
            ss[rows, :] = square if first else ss[rows, :] + square
            normed[rows, :] = (x * gain).astype(BF16)

        sweep((lo, hi), body)
        product = jnp.dot(
            normed[lo:hi, :], win[l, pl.ds(pl.multiple_of(block * F, 128), F), :],
            preferred_element_type=F32,
        )
        acc[lo:hi, :] = product if first else acc[lo:hi, :] + product

    def inner(l, a):
        lo, hi = span_in(l, a)
        absorb(l, t, a, True)
        ag_wait(l, mate, a)
        absorb(l, mate, a, False)
        for d in range(1, pairs):
            q = lax.rem(p + d, pairs)
            absorb(l, q * 2 + c, a, False)
            ag_wait(l, q * 2 + 1 - c, a)
            absorb(l, q * 2 + 1 - c, a, False)
        inverse = lax.rsqrt(jnp.sum(ss[lo:hi, :], axis=1, keepdims=True) / width + EPS)
        ext[l, HALO + lo : HALO + hi, :] = (acc[lo:hi, :] * inverse).astype(BF16)

    def halo_copy(l):
        return remote(
            ext.at[l, pl.ds(R, HALO), :], halo.at[l], hs_sem.at[l], hr_sem.at[l], {"sp": s + 1}
        )

    def halo_in(l):
        pl.when(s > 0)(lambda: halo_copy(l).wait_recv())

        @pl.when(s == 0)
        def _():
            ext[l, pl.ds(0, HALO), :] = jnp.zeros((HALO, group), BF16)

        @pl.when(s > 0)
        def _():
            ext[l, pl.ds(0, HALO), :] = halo[l]

    def pool(l, a):
        lo, hi = span_out(l, a)
        values = ext[l, lo : hi + HALO, :].astype(F32)
        two = values + pltpu.roll(values, 1, 0)
        four = two + pltpu.roll(two, 2, 0)
        eight = four + pltpu.roll(four, 4, 0)
        sixteen = eight + pltpu.roll(eight, 8, 0)
        total = jnp.where(t == 0, two, jnp.where(t == 1, four, jnp.where(t == 2, eight, sixteen)))
        window = jnp.where(t == 0, 2, jnp.where(t == 1, 4, jnp.where(t == 2, 8, 16)))
        place = s * R + lo + lax.broadcasted_iota(jnp.int32, (hi - lo, group), 0)
        count = jnp.minimum(place + 1, window).astype(F32)
        spread = (total[HALO:, :] / count - values[HALO:, :]).astype(BF16)
        mixed = jnp.dot(spread, w_pool[l, 0], preferred_element_type=F32)
        return (mixed * pool_scale[l : l + 1, :]).astype(BF16)

    def project(l, a, dest, mixed):
        lo, hi = span_out(l, a)
        for k in range(per):
            value = jnp.dot(mixed, wout[l, dest * per + k], preferred_element_type=F32)
            part[l, dest, lo:hi, k * cols_out : (k + 1) * cols_out] = value.astype(BF16)

    def pair_copy(l, q, a, i):
        lo, hi = bits(span_out(l, a))[i]
        rows, n = pl.ds(lo, hi - lo), a * 2 + i
        return remote(
            part.at[l, q * 2 + 1 - c, rows, :], pair.at[l, q, rows, :],
            ps_sem.at[l, q, n], pr_sem.at[l, q, n], {"tp": mate},
        )

    def cross_copy(l, q, slot, a, i):
        lo, hi = bits(span_out(l, a))[i]
        rows, n = pl.ds(lo, hi - lo), a * 2 + i
        return remote(
            summed.at[l, q, rows, :], xgot.at[l, slot, rows, :],
            xs_sem.at[l, q, n], xr_sem.at[l, slot, n], {"tp": q * 2 + c},
        )

    def scatter_first(l, a, mixed):
        for d in range(1, pairs):
            q = lax.rem(p + d, pairs)
            project(l, a, q * 2 + 1 - c, mixed)
            for i in range(2):
                pair_copy(l, q, a, i).start()
        for d in range(1, pairs):
            project(l, a, lax.rem(p + d, pairs) * 2 + c, mixed)

    def scatter_cross(l, a):
        for d in range(1, pairs):
            q = lax.rem(p + d, pairs)
            for i in range(2):
                pair_copy(l, q, a, i).wait_recv()

                def body(rows):
                    summed[l, q, rows, :] = (
                        part[l, q * 2 + c, rows, :].astype(F32) + pair[l, q, rows, :].astype(F32)
                    ).astype(BF16)

                sweep(bits(span_out(l, a))[i], body)
                cross_copy(l, q, p, a, i).start()

    def scatter_own(l, a, mixed):
        project(l, a, mate, mixed)
        for i in range(2):
            pair_copy(l, p, a, i).start()
        project(l, a, t, mixed)

    def sq_copy(l, slot, a, to):
        view = sq.at[l, a, slot]
        return remote(view, view, qs_sem.at[l, a, to], qr_sem.at[l, a, slot], {"tp": to})

    def settle(l, a):
        for i in range(2):
            pair_copy(l, p, a, i).wait_recv()
            for d in range(1, pairs):
                q = lax.rem(p + d, pairs)
                cross_copy(l, q, q, a, i).wait_recv()

            def add(rows):
                value = part[l, t, rows, :].astype(F32) + pair[l, p, rows, :].astype(F32)
                for d in range(1, pairs):
                    value = value + xgot[l, lax.rem(p + d, pairs), rows, :].astype(F32)
                branch[rows, :] = value
                ss[rows, :] = lanes(value * value)

            sweep(bits(span_out(l, a))[i], add)
        row = jnp.sum(jnp.transpose(ss[...]), axis=0, keepdims=True)
        sq[l, a, t] = jnp.broadcast_to(row, (8, R))
        for d in range(1, T):
            sq_copy(l, t, a, lax.rem(t + d, T)).start()
        tick()
        for d in range(1, T):
            other = lax.rem(t + d, T)
            sq_copy(l, other, a, other).wait_recv()
        squares = sq[l, a, 0]
        for k in range(1, T):
            squares = squares + sq[l, a, k]
        inverse = lax.rsqrt(squares / width + EPS)
        scale[...] = jnp.transpose(jnp.concatenate([inverse] * 16, axis=0))
        gain = gain_post[pl.ds(l, 1), pl.ds(pl.multiple_of(t * F, 128), F)]

        def update(rows):
            value = ag[l, t, rows, :].astype(F32) + branch[rows, :] * scale[rows, 0:1] * gain
            if l + 1 < layers:
                ag[l + 1, t, rows, :] = value.astype(BF16)
            else:
                out[rows, :] = value.astype(BF16)

        sweep(span_out(l, a), update)
        if l + 1 < layers:
            ag_start(l + 1, a)

    for m in range(M):
        load(m).start()
    barrier = pltpu.get_barrier_semaphore()

    def greet(where):
        pl.semaphore_signal(barrier, inc=1, device_id=where, device_id_type=MESH)

    pl.when(s < S - 1)(lambda: greet({"sp": s + 1}))
    pl.when(s > 0)(lambda: greet({"sp": s - 1}))
    if use_y:
        greet({"grp": 1 - g})
    for d in range(1, T):
        greet({"tp": lax.rem(t + d, T)})
    ag[0, t] = stream[...]
    ends = jnp.where(s > 0, 1, 0) + jnp.where(s < S - 1, 1, 0)
    pl.semaphore_wait(barrier, ends + (1 if use_y else 0) + T - 1)

    own(0)
    ag_start(0, 0)
    ag_start(0, 1)
    each = (S - 1) * PIECES
    for l in range(layers):
        if l == 0:
            tick(each // 3)
            ag_relay(0, 0)
            tick(each // 3)
            ag_relay(0, 1)
        else:
            ag_relay(l, 0)
        pump(2 * l)
        finish(2 * l)
        inner(l, 0)
        pl.when(s < S - 1)(lambda: halo_copy(l).start())
        mixed = pool(l, 0)
        if l == 0:
            tick()
            inner(l, 1)
            tick()
            halo_in(l)
            later = pool(l, 1)
        pump(2 * l + 1)
        finish(2 * l + 1)
        scatter_first(l, 0, mixed)
        tick()
        if l > 0:
            ag_relay(l, 1)
        scatter_cross(l, 0)
        tick()
        scatter_own(l, 0, mixed)
        tick()
        if l > 0:
            inner(l, 1)
            tick()
            halo_in(l)
            later = pool(l, 1)
        scatter_first(l, 1, later)
        tick()
        scatter_cross(l, 1)
        tick()
        scatter_own(l, 1, later)
        tick()
        settle(l, 0)
        tick()
        settle(l, 1)
        tick()

    for l in range(layers):
        pl.when(s < S - 1)(lambda: halo_copy(l).wait_send())
        for a in range(2):
            for d in range(1, T):
                sq_copy(l, t, a, lax.rem(t + d, T)).wait_send()
            for i in range(2):
                n = a * 2 + i
                for q in range(pairs):
                    ag_copy(l, t, a, i, agp_sem.at[l, q, n], mate).wait_send()
                    pair_copy(l, q, a, i).wait_send()
                for d in range(1, pairs):
                    q = lax.rem(p + d, pairs)
                    ag_copy(l, t, a, i, agx_sem.at[l, q, n], mate).wait_send()
                    cross_copy(l, q, p, a, i).wait_send()
    for m in range(M):
        for src in range(S):
            for h in range(PIECES):
                pl.when(jnp.logical_and(src <= s, s < S - 1))(lambda: z_copy(m, src, 0, h).wait_send())
                pl.when(jnp.logical_and(src >= s, s > 0))(lambda: z_copy(m, src, 1, h).wait_send())
                if use_y:
                    pl.when(s != src)(lambda: y_copy(m, src, h).wait_send())


def per_device(G, S, T, stream, gain_pre, w_in, w_pool, pool_scale, w_out, gain_post):
    layers, width = gain_pre.shape
    R, F = stream.shape
    group = w_pool.shape[2]
    pairs = T // 2
    M = 2 * layers
    dma = pltpu.SemaphoreType.DMA
    vmem = pl.BlockSpec(memory_space=pltpu.VMEM)
    anywhere = pl.BlockSpec(memory_space=pl.ANY)
    return pl.pallas_call(
        functools.partial(kernel, G, S, T, layers, width),
        out_shape=jax.ShapeDtypeStruct((R, F), BF16),
        in_specs=[vmem, vmem, anywhere, vmem, vmem, anywhere, vmem],
        out_specs=vmem,
        scratch_shapes=[
            pltpu.VMEM((layers, width, group), BF16),
            pltpu.VMEM((layers, S, group, w_out.shape[2]), BF16),
            pltpu.VMEM((layers, T, R, F), BF16),
            pltpu.VMEM((layers, T, R, F), BF16),
            pltpu.VMEM((layers, pairs, R, F), BF16),
            pltpu.VMEM((layers, pairs, R, F), BF16),
            pltpu.VMEM((layers, pairs, R, F), BF16),
            pltpu.VMEM((R, F), BF16),
            pltpu.VMEM((R, group), F32),
            pltpu.VMEM((R, 128), F32),
            pltpu.VMEM((R, 128), F32),
            pltpu.VMEM((R, F), F32),
            pltpu.VMEM((layers, HALO + R, group), BF16),
            pltpu.VMEM((layers, HALO, group), BF16),
            pltpu.VMEM((layers, 2, T, 8, R), F32),
            dma((M,)),
            dma((M, S, 2, PIECES)),
            dma((M, S, PIECES)),
            dma((M, S, PIECES)),
            dma((M, S, PIECES)),
            dma((layers, pairs, CHUNKS)),
            dma((layers, pairs, CHUNKS)),
            dma((layers, T, CHUNKS)),
            dma((layers, pairs, CHUNKS)),
            dma((layers, pairs, CHUNKS)),
            dma((layers, pairs, CHUNKS)),
            dma((layers, pairs, CHUNKS)),
            dma((layers, 2, T)),
            dma((layers, 2, T)),
            dma((layers,)),
            dma((layers,)),
        ],
        compiler_params=pltpu.CompilerParams(
            collective_id=0, has_side_effects=True, vmem_limit_bytes=60 * 1024 * 1024
        ),
    )(stream, gain_pre, w_in, w_pool, pool_scale, w_out, gain_post)


def plane_kernel(
    G, S, T, layers, width, order,
    stream_hbm, gain_pre_hbm, w_in, w_pool, scale_hbm, w_out, gain_post_hbm,
    out,
    stream, gain_pre, gain_post, win, wout, wp, scales, rows_in, x, held,
    part, got, far, edge, psq, esq, mix, branch, bsq,
    load_sem, small_sem, self_sem, y_send, y_recv, x_send, x_recv, f_send, f_recv,
    wo_send, wo_recv, wx_send, wx_recv, wy_send, wy_recv, wf_send, wf_recv,
    p_send, p_recv, c_send, c_recv,
    r_send, r_recv, o_send, o_recv, rq_send, rq_recv, h_send, h_recv, hq_send, hq_recv, m_send, m_recv, mq_send, mq_recv,
):
    g, s, t = lax.axis_index("grp"), lax.axis_index("sp"), lax.axis_index("tp")
    pairs = T // 2
    p, c = lax.div(t, 2), lax.rem(t, 2)
    mate = p * 2 + 1 - c
    R, F = stream.shape
    C = R // T
    group = w_pool.shape[2]
    sides = 2 if G == 2 else 1
    side = g if sides == 2 else 0
    M = 2 * layers
    line_width = psq.shape[-1]
    H = S // 2
    low = lax.div(s, H) * H
    here = s - low
    hub, far_hub = jnp.where(low == 0, H - 1, H), jnp.where(low == 0, H, H - 1)
    is_hub = s == hub
    near = [low + lax.rem(here + d, H) for d in range(1, H)]
    away = [H - low + d for d in range(H)]
    spread_order = [jnp.where(low == 0, H - 1 - d, d) for d in range(H)]
    planes = near + away

    def slot(k):
        return lax.rem(k - low + S, S)

    def remote(src, dst, send, recv, where):
        return pltpu.make_async_remote_copy(
            src_ref=src, dst_ref=dst, send_sem=send, recv_sem=recv,
            device_id=where, device_id_type=MESH,
        )

    def sent(view, sem):
        remote(view, view, sem, sem, {"tp": mate}).wait_send()

    def landed(view, sem):
        remote(view, view, sem, sem, {"tp": mate}).wait_recv()

    barrier = pltpu.get_barrier_semaphore()

    def greet(where):
        pl.semaphore_signal(barrier, inc=1, device_id=where, device_id_type=MESH)

    for ds in range(S):
        for dt in range(T):
            if ds or dt:
                greet({"sp": lax.rem(s + ds, S), "tp": lax.rem(t + dt, T)})
    if sides == 2:
        greet({"grp": 1 - g})

    smalls = [
        pltpu.make_async_copy(stream_hbm, stream, small_sem.at[0]),
        pltpu.make_async_copy(gain_pre_hbm, gain_pre, small_sem.at[1]),
        pltpu.make_async_copy(gain_post_hbm, gain_post, small_sem.at[2]),
    ]
    scale_load = pltpu.make_async_copy(scale_hbm, scales, small_sem.at[3])

    def block(m, k):
        if m % 2 == 0:
            return win.at[m // 2, slot(k)]
        return wout.at[m // 2, pl.ds(pl.multiple_of(slot(k) * group, 16), group), :]

    def piece(m, k, half, h):
        rows = (F if m % 2 == 0 else group) // sides
        length = rows // PARTS
        start = half * rows + h * length
        if m % 2 == 0:
            return win.at[m // 2, slot(k), pl.ds(pl.multiple_of(start, 16), length), :]
        return wout.at[m // 2, pl.ds(pl.multiple_of(slot(k) * group + start, 16), length), :]

    def load(m):
        return pltpu.make_async_copy((w_out if m % 2 else w_in).at[m // 2], block(m, t), load_sem.at[m])

    def own_copy(m, k):
        return remote(block(m, k), block(m, k), wo_send.at[m], wo_recv.at[m], {"tp": mate})

    def cross_copy(m, k, d, q, h):
        view = piece(m, k, side, h)
        return remote(view, view, wx_send.at[m, d], wx_recv.at[m, d, h], {"tp": q * 2 + c})

    def grp_copy(m, d, q, half, h):
        view = piece(m, q * 2 + c, half, h)
        return remote(view, view, wy_send.at[m, d], wy_recv.at[m, d, h], {"grp": 1 - g})

    def mate_copy(m, d, q, half, h):
        view = piece(m, q * 2 + c, half, h)
        return remote(view, view, wf_send.at[m, d], wf_recv.at[m, d], {"tp": mate})

    others = [(d, lax.rem(p + 1 + d, pairs)) for d in range(pairs - 1)]

    def weight_own(m):
        load(m).wait()
        own_copy(m, t).start()

    def weight_cross(m, h):
        for d, q in others:
            back = pairs - 2 - d
            view = piece(m, t, side, h)
            remote(view, view, wx_send.at[m, d], wx_recv.at[m, back, h], {"tp": q * 2 + c}).start()

    def weight_relay(m, h):
        for d, q in others:
            cross_copy(m, q * 2 + c, d, q, h).wait_recv()
            if sides == 2:
                grp_copy(m, d, q, side, h).start()
            mate_copy(m, d, q, side, h).start()

    def weight_second(m, h):
        if sides == 2:
            for d, q in others:
                grp_copy(m, d, q, 1 - side, h).wait_recv()
                mate_copy(m, d, q, 1 - side, h).start()

    def weight_last(m):
        for d, q in others:
            landed(block(m, q * 2 + 1 - c), wf_recv.at[m, d])

    def share(m, k):
        rows = (F if m % 2 == 0 else group) // sides
        if m % 2 == 0:
            return win.at[m // 2, slot(k), pl.ds(0, rows), :]
        return wout.at[m // 2, pl.ds(pl.multiple_of(slot(k) * group, 16), rows), :]

    def pool_copy(l, d):
        return remote(wp.at[l], wp.at[l], p_send.at[d - 1], p_recv.at[l], {"tp": lax.rem(t + d, T)})

    def scale_copy(d):
        return remote(scales, scales, c_send.at[d - 1], c_recv, {"tp": lax.rem(t + d, T)})

    def pool_send(l):
        @pl.when(t == s)
        def _():
            for d in range(1, T):
                pool_copy(l, d).start()

    def lanes(v):
        return sum(v[:, i : i + 128] for i in range(0, F, 128))

    def line(square):
        if C < line_width:
            square = jnp.concatenate([square, jnp.zeros((line_width - C, 128), F32)], axis=0)
        row = jnp.sum(jnp.transpose(square), axis=0, keepdims=True)
        return jnp.broadcast_to(row, (8, line_width))

    def column(values, first=0):
        return jnp.transpose(jnp.concatenate([values] * 16, axis=0))[first:C]

    def wide(values, n):
        return jnp.concatenate([values] * (n // 128), axis=1)

    def squares_start(ref, l, q, send, recv):
        for d in range(1, S):
            remote(ref.at[l, q, 0], ref.at[l, q, d], send, recv.at[q], {"sp": lax.rem(s + d, S)}).start()

    def squares_wait(ref, l, q, recv):
        landed(ref.at[l, q, pl.ds(1, S - 1)], recv.at[q])

    def total(ref, l, q):
        return sum(ref[l, q, k] for k in range(S))

    def next_run(l, q, start):
        if q + 1 < S:
            start(q + lax.div(t + 1, T), 0)
        else:
            pl.when(t + 1 < T)(lambda: start(q, 1))

    def edge_copy(l, q, k, index, plane, final):
        def start(ahead, last):
            remote(
                part.at[l, q, k, pl.ds(C - HALO, HALO), :], edge.at[l, ahead, index],
                h_send.at[2 * final + last], h_recv.at[l, ahead], {"sp": plane, "tp": lax.rem(t + 1, T)},
            ).start()

        next_run(l, q, start)

    def edge_squares(l, q):
        def start(ahead, last):
            for d in range(S):
                remote(
                    psq.at[l, q, 0], esq.at[l, ahead, d], hq_send.at[last], hq_recv.at[l, ahead],
                    {"sp": lax.rem(s + d, S), "tp": lax.rem(t + 1, T)},
                ).start()

        next_run(l, q, start)

    step = C // CUTS

    def run_copy(to, origin, n):
        rows = pl.ds(pl.multiple_of(to * C + n * step, 16), step)
        return remote(
            stream.at[rows, :], rows_in.at[origin, pl.ds(n * step, step)],
            y_send, y_recv.at[origin, n], {"tp": to},
        )

    def run_landed(origin, n):
        landed(rows_in.at[origin, pl.ds(n * step, step)], y_recv.at[origin, n])

    def run_of(f, n, local):
        if local:
            return stream.at[pl.ds(pl.multiple_of(t * C + n * step, 16), step), :]
        return rows_in.at[f, pl.ds(n * step, step)]

    def stream_on(f, n, local=False):
        view = x.at[s, pl.ds(n * step, step)]
        pl.when(f == s)(lambda: pltpu.make_async_copy(run_of(f, n, local), view, self_sem.at[0]).start())
        pl.when(f != s)(lambda: remote(run_of(f, n, local), view, x_send, x_recv.at[s], {"sp": f}).start())

    def stream_self_wait():
        pltpu.make_async_copy(rows_in.at[s], x.at[s], self_sem.at[0]).wait()

    def final_copy(q):
        rows = pl.ds(pl.multiple_of(t * C, 16), C)
        return remote(x.at[q], out.at[rows, :], f_send, f_recv, {"sp": q, "tp": s})

    def final_self(q):
        rows = pl.ds(pl.multiple_of(t * C, 16), C)
        return pltpu.make_async_copy(x.at[q], out.at[rows, :], self_sem.at[1])

    def features(ref, l):
        return ref[pl.ds(l, 1), pl.ds(pl.multiple_of(s * F, 128), F)]

    def stage_a(l, q):
        with jax.named_scope(f"a{l}{q}"):
            advance(l, q)

    def advance(l, q):
        if l == 0:
            pl.when(s == q)(stream_self_wait)
            pl.when(s != q)(lambda: landed(x.at[q], x_recv.at[q]))
            value = x[q].astype(F32)
        else:
            squares_wait(bsq, l - 1, q, mq_recv)
            inverse = column(lax.rsqrt(total(bsq, l - 1, q) / width + EPS))
            new = x[q].astype(F32) + branch[q] * wide(inverse, F) * features(gain_post, l - 1)
            new = new.astype(BF16)
            x[q] = new
            if l == layers:
                return
            value = new.astype(F32)
        scaled = (value * features(gain_pre, l)).astype(BF16)
        if l == 0:
            held[q] = scaled
            pl.when(p == low // H)(lambda: inward(l, q, scaled))
            pl.when(p != low // H)(lambda: outward(l, q, scaled))
        else:
            if q == 0:
                ready(2 * l)
            outward(l, q, scaled)
        psq[l, q, 0] = line(lanes(value * value))
        squares_start(psq, l, q, rq_send, rq_recv)
        edge_squares(l, q)
        if l > 0:
            inward(l, q, scaled)

    def stage_e(q):
        with jax.named_scope(f"e{q}"):
            pl.when(p == low // H)(lambda: outward(0, q, held[q]))
            pl.when(p != low // H)(lambda: inward(0, q, held[q]))

    def weight_first():
        with jax.named_scope("first"):
            weight_last(0)

    def stage_z(q):
        mine = jnp.logical_and(s == q, t == s)
        pl.when(mine)(lambda: final_self(q).start())
        pl.when(jnp.logical_not(mine))(lambda: final_copy(q).start())

    def project(l, q, k, scaled):
        part[l, q, k] = jnp.dot(scaled, win[l, k], preferred_element_type=F32).astype(BF16)

    def outward(l, q, scaled):
        index = jnp.where(here > hub - low, here - 1, here)
        for j, k in enumerate(spread_order):
            project(l, q, H + k, scaled)
            pl.when(jnp.logical_not(is_hub))(
                lambda j=j, k=k: remote(
                    part.at[l, q, H + k], far.at[l, q, index, k], o_send, o_recv.at[j, q], {"sp": hub}
                ).start()
            )

    def inward(l, q, scaled):
        for k in range(H):
            project(l, q, k, scaled)
        for d, k in enumerate(near):
            remote(
                part.at[l, q, slot(k)], got.at[l, q, H - 2 - d], r_send, r_recv.at[q], {"sp": k}
            ).start()
            edge_copy(l, q, slot(k), H - 2 - d, k, 0)
        edge_copy(l, q, here, H, s, 0)

    def stage_s(l, q):
        with jax.named_scope(f"s{l}{q}"):

            @pl.when(is_hub)
            def _():
                for j, k in enumerate(spread_order):
                    landed(far.at[l, q, pl.ds(0, H - 1), k], o_recv.at[j, q])
                    value = part[l, q, H + k].astype(F32)
                    for d in range(H - 1):
                        value = value + far[l, q, d, k].astype(F32)
                    part[l, q, H + k] = value.astype(BF16)
                    remote(
                        part.at[l, q, H + k], got.at[l, q, H - 1], o_send, r_recv.at[q], {"sp": H - low + k}
                    ).start()
                    edge_copy(l, q, H + k, H - 1, H - low + k, 1)

    def ready(m):
        landed(block(m, mate), wo_recv.at[m])
        weight_last(m)

    def stage_b(l, q):
        with jax.named_scope(f"b{l}{q}"):
            smooth(l, q)

    def smooth(l, q):
        squares_wait(psq, l, q, rq_recv)
        inverse = column(lax.rsqrt(total(psq, l, q) / width + EPS))

        def arrived():
            landed(esq.at[l, q], hq_recv.at[l, q])
            landed(edge.at[l, q], h_recv.at[l, q])

        if q == 0:
            pl.when(t > 0)(arrived)
            pl.when(t != s)(lambda: landed(wp.at[l], p_recv.at[l]))
            if l == 0:
                pl.when(t != s)(lambda: landed(scales, c_recv))
        else:
            arrived()
        before = column(lax.rsqrt(total(esq, l, q) / width + EPS), C - HALO)
        ahead = sum(edge[l, q, k].astype(F32) for k in range(H + 1))
        landed(got.at[l, q], r_recv.at[q])
        value = part[l, q, here].astype(F32)
        for k in range(H):
            value = value + got[l, q, k].astype(F32)
        values = jnp.concatenate([ahead * wide(before, group), value * wide(inverse, group)], axis=0)
        values = values.astype(BF16).astype(F32)
        reach = values
        pooled = values
        for k in range(S):
            reach = reach + pltpu.roll(reach, 2**k, 0)
            pooled = jnp.where(s == k, reach, pooled)
        window = jnp.left_shift(2, s)
        place = q * R + t * C + lax.broadcasted_iota(jnp.int32, (C, group), 0)
        count = jnp.minimum(place + 1, window).astype(F32)
        spread = (pooled[HALO:, :] / count - values[HALO:, :]).astype(BF16)
        mixed = jnp.dot(spread, wp[l], preferred_element_type=F32)
        mix[l, q, here] = (mixed * scales[l : l + 1, :]).astype(BF16)

        def on(k, kind):
            lower = lax.div(k, H) * H
            remote(
                mix.at[l, q, here], mix.at[l, q, lax.rem(s - lower + S, S)],
                m_send.at[3 if kind else 0], m_recv.at[kind, q], {"sp": k},
            ).start()

        for k in near if RELAYED else planes:
            on(k, 0)
        if RELAYED:
            pl.when(is_hub)(lambda: on(far_hub, 1))

    def mates_view(l, q):
        return mix.at[l, q, pl.ds(0, H - 1)]

    def stage_f(l, q):
        with jax.named_scope(f"f{l}{q}"):

            @pl.when(is_hub)
            def _():
                landed(mates_view(l, q), m_recv.at[0, q])
                for j in range(1, H):
                    from_here = lax.rem(here + j, H)
                    for k in [H - low + d for d in spread_order]:
                        remote(
                            mix.at[l, q, from_here], mix.at[l, q, H + from_here],
                            m_send.at[1], m_recv.at[2, q], {"sp": k},
                        ).start()

    def stage_g(l, q):
        with jax.named_scope(f"g{l}{q}"):

            @pl.when(is_hub)
            def _():
                spot = slot(far_hub)
                landed(mix.at[l, q, spot], m_recv.at[1, q])
                for k in near:
                    remote(
                        mix.at[l, q, spot], mix.at[l, q, spot],
                        m_send.at[2], m_recv.at[1, q], {"sp": k},
                    ).start()

    def stage_d(l, q):
        with jax.named_scope(f"d{l}{q}"):
            if q == 0:
                ready(2 * l + 1)

            if RELAYED:

                @pl.when(jnp.logical_not(is_hub))
                def _():
                    landed(mates_view(l, q), m_recv.at[0, q])
                    landed(mix.at[l, q, 0], m_recv.at[1, q])

                landed(mates_view(l, q), m_recv.at[2, q])
            else:
                landed(mix.at[l, q, pl.ds(0, S - 1)], m_recv.at[0, q])
            value = jnp.dot(
                jnp.concatenate([mix[l, q, k] for k in range(S)], axis=1), wout[l],
                preferred_element_type=F32,
            )
            branch[q] = value
            bsq[l, q, 0] = line(lanes(value * value))
            squares_start(bsq, l, q, mq_send, mq_recv)

    smalls[0].start()
    for m in range(M):
        load(m).start()
    smalls[1].start()
    smalls[2].start()
    pool_load = [pltpu.make_async_copy(w_pool.at[l, 0], wp.at[l], p_recv.at[l]) for l in range(layers)]

    @pl.when(t == s)
    def _():
        for l in range(layers):
            pool_load[l].start()
        scale_load.start()

    @pl.when(t == 0)
    def _():
        for l in range(layers):
            edge[l, 0] = jnp.zeros(edge.shape[2:], BF16)
            esq[l, 0] = jnp.zeros(esq.shape[2:], F32)

    smalls[0].wait()
    pl.semaphore_wait(barrier, S * T - 1 + (1 if sides == 2 else 0))

    for n in range(CUTS):
        for _, q in others:
            run_copy(q * 2 + c, t, n).start()
            run_copy(q * 2 + 1 - c, t, n).start()
    for n in range(CUTS):
        run_copy(mate, t, n).start()
        stream_on(t, n, True)
    weight_own(0)
    for h in range(PARTS):
        weight_cross(0, h)
    weight_own(1)
    for h in range(PARTS):
        weight_cross(1, h)
    with jax.named_scope("enter"):
        for n in range(CUTS):
            run_landed(mate, n)
            stream_on(mate, n)
        for n in range(CUTS):
            for _, q in others:
                for core in (c, 1 - c):
                    run_landed(q * 2 + core, n)
                    stream_on(q * 2 + core, n)
        for h in range(PARTS):
            weight_relay(0, h)
    landed(block(0, mate), wo_recv.at[0])

    @pl.when(t == s)
    def _():
        for l in range(layers):
            pool_load[l].wait()
        scale_load.wait()
        for d in range(1, T):
            scale_copy(d).start()

    pool_send(0)
    smalls[1].wait()
    smalls[2].wait()

    actions = (
        stage_a, stage_b, None, stage_d, weight_own, pool_send, weight_cross, weight_relay, weight_second,
        stage_s, stage_f, stage_g, stage_z, stage_e, weight_first,
    )
    for kind, *where in order:
        actions[kind](*where)

    rows = pl.ds(0, (T - 1) * C)

    @pl.when(s == t)
    def _():
        final_self(s).wait()
        landed(out.at[rows, :], f_recv)
        sent(out.at[rows, :], f_send)

    @pl.when(s != t)
    def _():
        landed(out, f_recv)
        sent(out, f_send)

    with jax.named_scope("drain"):
        sent(stream.at[rows, :], y_send)
        sent(x.at[pl.ds(0, S - 1)], x_send)

        @pl.when(t == s)
        def _():
            for d in range(1, T):
                sent(scales, c_send.at[d - 1])
                sent(wp, p_send.at[d - 1])

        for m in range(M):
            sent(block(m, t), wo_send.at[m])
            for d, q in others:
                sent(share(m, t), wx_send.at[m, d])
                sent(block(m, t), wf_send.at[m, d])
                if sides == 2:
                    sent(share(m, t), wy_send.at[m, d])
        sent(psq.at[:, :, pl.ds(0, S - 1)], rq_send)
        sent(bsq.at[:, :, pl.ds(0, S - 1)], mq_send)
        sent(part.at[:, :, pl.ds(0, H - 1)], r_send)
        sent(part.at[:, :, pl.ds(0, H)], o_send)
        sent(mix.at[:, :, pl.ds(0, (H if RELAYED else S) - 1)], m_send.at[0])

        @pl.when(is_hub if RELAYED else s < 0)
        def _():
            sent(mix.at[:, :, 0], m_send.at[3])
            sent(mix.at[:, :, pl.ds(0, (H - 1) * H)], m_send.at[1])
            sent(mix.at[:, :, pl.ds(0, H - 1)], m_send.at[2])

        sent(edge.at[:, pl.ds(0, S - 1), pl.ds(0, H)], h_send.at[0])
        sent(esq.at[:, pl.ds(0, S - 1)], hq_send.at[0])
        pl.when(is_hub)(lambda: sent(edge.at[:, pl.ds(0, S - 1), pl.ds(0, H)], h_send.at[2]))

        @pl.when(t + 1 < T)
        def _():
            sent(edge.at[:, 0, pl.ds(0, H)], h_send.at[1])
            sent(esq.at[:, 0], hq_send.at[1])
            pl.when(is_hub)(lambda: sent(edge.at[:, 0, pl.ds(0, H)], h_send.at[3]))


def stage_order(layers, runs):
    steps = []
    begins = {0: 0, 9: AT_S, 1: AT_B, 3: AT_D}
    if RELAYED:
        begins |= {10: AT_F, 11: AT_G}
    steps.append((-90, (14,)))
    for h in range(PARTS):
        steps.append((-100 + EARLY[0] + h * EARLY[1], (8, 0, h)))
    for l in range(layers + 1):
        for kind, at in begins.items():
            if l < layers or kind == 0:
                for q in range(runs):
                    pace = STRIDES[0 if l == 0 else 1 if l + 1 < layers else 2]
                    if l == 0 and kind == 0:
                        steps.append((q - 100, (0, 0, q)))
                        steps.append((q * pace, (13, q)))
                    else:
                        steps.append((l * PERIOD + at + q * pace, (kind, l, q)))
    last = max(at for at, step in steps if step[0] == 3)
    for at, step in list(steps):
        if step[:2] == (0, layers):
            steps.append((max(at, last + AT_Z) + 0.01, (12, step[2])))
    for m in range(1, 2 * layers):
        due = m // 2 * PERIOD + (AT_D if m % 2 else 0) - 0.1
        odd = m % 2
        begin = due - LEADS[odd]
        relay, second = RELAYS[odd], SECONDS[odd]
        if m == 1:
            relay, second = FIRST
            begin = due - (PARTS - 1) * SPACE - relay - second
        for h in range(PARTS):
            if m > 1:
                if h == 0:
                    steps.append((begin, (4, m)))
                    if m % 2 == 0:
                        steps.append((begin, (5, m // 2)))
                steps.append((begin + h * SPACE, (6, m, h)))
            steps.append((begin + h * SPACE + relay, (7, m, h)))
            steps.append((begin + h * SPACE + relay + second, (8, m, h)))
    return [step for _, step in sorted(steps)]


def per_plane(G, S, T, stream, gain_pre, w_in, w_pool, pool_scale, w_out, gain_post):
    layers, width = gain_pre.shape
    R, F = stream.shape
    group = w_pool.shape[2]
    C = R // T
    H = S // 2
    pairs = T // 2
    M = 2 * layers
    wide = max(128, C)
    dma = pltpu.SemaphoreType.DMA
    anywhere = pl.BlockSpec(memory_space=pl.ANY)
    return pl.pallas_call(
        functools.partial(plane_kernel, G, S, T, layers, width, stage_order(layers, S)),
        out_shape=jax.ShapeDtypeStruct((R, F), BF16),
        in_specs=[anywhere] * 7,
        out_specs=OUT_SPEC,
        scratch_shapes=[
            pltpu.VMEM((R, F), BF16),
            pltpu.VMEM((layers, width), F32),
            pltpu.VMEM((layers, width), F32),
            pltpu.VMEM((layers, T, F, group), BF16),
            pltpu.VMEM((layers, T * group, F), BF16),
            pltpu.VMEM((layers, group, group), BF16),
            pltpu.VMEM((layers, group), F32),
            pltpu.VMEM((T, C, F), BF16),
            pltpu.VMEM((S, C, F), BF16),
            pltpu.VMEM((S, C, F), BF16),
            pltpu.VMEM((layers, S, S, C, group), BF16),
            pltpu.VMEM((layers, S, H, C, group), BF16),
            pltpu.VMEM((layers, S, H - 1, H, C, group), BF16),
            pltpu.VMEM((layers, S, H + 1, HALO, group), BF16),
            pltpu.VMEM((layers, S, S, 8, wide), F32),
            pltpu.VMEM((layers, S, S, 8, wide), F32),
            pltpu.VMEM((layers, S, S, C, group), BF16),
            pltpu.VMEM((S, C, F), F32),
            pltpu.VMEM((layers, S, S, 8, wide), F32),
            dma((M,)),
            dma((4,)),
            dma((2,)),
            dma(()),
            dma((T, CUTS)),
            dma(()),
            dma((S,)),
            dma(()),
            dma(()),
            dma((M,)),
            dma((M,)),
            dma((M, pairs - 1)),
            dma((M, pairs - 1, PARTS)),
            dma((M, pairs - 1)),
            dma((M, pairs - 1, PARTS)),
            dma((M, pairs - 1)),
            dma((M, pairs - 1)),
            dma((T - 1,)),
            dma((layers,)),
            dma((T - 1,)),
            dma(()),
            dma(()),
            dma((S,)),
            dma(()),
            dma((H, S)),
            dma(()),
            dma((S,)),
            dma((4,)),
            dma((layers, S)),
            dma((2,)),
            dma((layers, S)),
            dma((4,)),
            dma((3, S)),
            dma(()),
            dma((S,)),
        ],
        compiler_params=pltpu.CompilerParams(
            collective_id=0, has_side_effects=True, vmem_limit_bytes=60 * 1024 * 1024
        ),
    )(stream, gain_pre, w_in, w_pool, pool_scale, w_out, gain_post)


def plan(G, S, T, *args):
    stream, w_pool = args[0], args[3]
    planes = S == T == T * w_pool.shape[1] and S // 2 == T // 2 == 2 and stream.shape[0] % (HALO * CUTS * T) == 0
    return (per_plane if planes else per_device)(G, S, T, *args)


def solution(mesh):
    G, S, T = mesh.shape["grp"], mesh.shape["sp"], mesh.shape["tp"]
    return jax.shard_map(
        functools.partial(plan, G, S, T),
        mesh=mesh,
        in_specs=(
            P(("grp", "sp"), "tp"),
            P(),
            P(None, "sp", "tp"),
            P(None, "tp", None, None),
            P(None, "tp"),
            P(None, "tp", "sp"),
            P(),
        ),
        out_specs=P(("grp", "sp"), "tp"),
        check_vma=False,
    )
```
